128 devices in a mesh: fs: 16 (over z, y), tp: 8 (over x, core).
Axes of the slice: x: 4, y: 4, z: 4, core: 2. Of those that a mesh axis runs over, the one named last changes fastest.
Arguments:
- query_latent_rows: bfloat16 [24576, 1024], P('fs'), may hold values from -6 to 6
- grad_q: bfloat16 [24576, 3072], P('fs', 'tp'), may hold values from -6 to 6
- head_out: bfloat16 [24576, 2048], P('fs', 'tp'), may hold values from -6 to 6
- grad_out: bfloat16 [24576, 4096], P('fs'), may hold values from -6 to 6
- proj_q: bfloat16 [1024, 256], P('fs'), may hold values from -0.5 to 0.5
- proj_o: bfloat16 [4096, 256], P('fs'), may hold values from -0.5 to 0.5
- query_up_weight: float32 [1024, 3072], P('fs', 'tp'), may hold values from -0.1875 to 0.1875
- weight_o: float32 [4096, 2048], P('fs', 'tp'), may hold values from -0.125 to 0.125
- first_q: float32 [256, 3072], P('fs', 'tp'), may hold values from -6 to 6
- second_q: float32 [256, 3072], P('fs', 'tp'), may hold values from 0.25 to 4
- first_o: float32 [256, 2048], P('fs', 'tp'), may hold values from -6 to 6
- second_o: float32 [256, 2048], P('fs', 'tp'), may hold values from 0.25 to 4
Outputs:
- new_weight_q: float32 [1024, 3072], P('fs', 'tp')
- new_weight_o: float32 [4096, 2048], P('fs', 'tp')
- new_first_q: float32 [256, 3072], P('fs', 'tp')
- new_second_q: float32 [256, 3072], P('fs', 'tp')
- new_first_o: float32 [256, 2048], P('fs', 'tp')
- new_second_o: float32 [256, 2048], P('fs', 'tp')
- step_q: float32 [1024, 3072], P('fs', 'tp')
- step_o: float32 [4096, 2048], P('fs', 'tp')
- copy_q: bfloat16 [1024, 3072], P(None, 'tp')
- copy_o: bfloat16 [4096, 2048], P(None, 'tp')
The draws below stay inside these ranges and needn't reach their ends.
All inputs are finite; a program needn't handle non-finite values.
Results may differ from the reference program's by a relative error of at most 0.008.
Values may be sent and summed in bfloat16 or wider, within the bound.
A program may use at most 128 MiB of HBM per device.

```python
import math
import jax
import jax.numpy as jnp
from jax import lax

D = 4096
QUERY_LATENT = 1024
RANK = 256
QUERY_COLUMNS = 3072
BW = 2048
TOKEN_TOTAL = 24576


def reduced_basis(key, height):
    column = jnp.arange(RANK, dtype=jnp.float32)
    falloff = 10.0 ** (-column / RANK)
    entries = jnp.clip(jax.random.normal(key, (height, RANK), jnp.float32), -4.0, 4.0)
    return (entries * falloff[None, :] / math.sqrt(height)).astype(jnp.bfloat16)


def draw_proj_q(key, part):
    return reduced_basis(jax.random.fold_in(key, 11), QUERY_LATENT)


def draw_proj_o(key, part):
    return reduced_basis(jax.random.fold_in(key, 12), D)


def raised(drawn, stream_key, source, target, shards_of, factor):
    def block_of(axis_at):
        return (jnp.arange(drawn.shape[axis_at]) // (drawn.shape[axis_at] // shards_of)).reshape((-1,) + (1,) * (drawn.ndim - 1 - axis_at))

    one_side = jax.random.permutation(stream_key, shards_of)[block_of(target)]
    far = (block_of(target) + shards_of // 2) % shards_of
    return jnp.where((block_of(source) == one_side) | (block_of(source) == far), factor * drawn, drawn)


def steps_of(key, extent, cuts, smallest, largest):
    loudness, own = 1.0, jax.random.fold_in(key, 6)
    for axis_at, shards_of in cuts:
        heights = jnp.exp(jax.random.uniform(jax.random.fold_in(own, axis_at), (shards_of,), jnp.float32, smallest / len(cuts), largest / len(cuts)))
        loudness = loudness * jnp.repeat(heights, extent[axis_at] // shards_of).reshape([-1 if axis == axis_at else 1 for axis in range(len(extent))])
    return loudness


def scatter_about(stream_key, shape, deviation, most, split=(), held_as=jnp.bfloat16):
    array = deviation * jax.random.normal(stream_key, shape, jnp.float32)
    if split:
        array = array * steps_of(stream_key, shape, split, -0.22, 0.18)
    return jnp.clip(array, -most, most).astype(held_as)


def noise_with(rng, shape, spread, limit, pieces, heavy, held_as=jnp.bfloat16):
    result = spread * jax.random.normal(rng, shape, jnp.float32)
    if pieces:
        result = result * steps_of(rng, shape, pieces, -0.22, 0.18)
    return jnp.clip(raised(result, jax.random.fold_in(rng, 3), *heavy), -limit, limit).astype(held_as)


def setup_inputs(seed: int = 0) -> dict:
    streams_of = jax.random.split(jax.random.key(seed), 13)
    query_latent_rows = noise_with(streams_of[0], (TOKEN_TOTAL, QUERY_LATENT), 1.0, 6.0, ((0, 16),), (0, 1, 16, 2.0))
    grad_q = scatter_about(streams_of[1], (TOKEN_TOTAL, QUERY_COLUMNS), 1.0, 6.0, ((0, 16), (1, 8)))
    head_out = scatter_about(streams_of[2], (TOKEN_TOTAL, BW), 1.0, 6.0, ((0, 16), (1, 8)))
    grad_out = noise_with(streams_of[3], (TOKEN_TOTAL, D), 1.0, 6.0, ((0, 16),), (0, 1, 16, 2.0))
    proj_q = draw_proj_q(jax.random.fold_in(streams_of[12], 71), 0)
    proj_o = draw_proj_o(jax.random.fold_in(streams_of[12], 71), 0)
    query_up_weight = scatter_about(streams_of[6], (QUERY_LATENT, QUERY_COLUMNS), QUERY_LATENT ** -0.5, 0.1875, ((0, 16), (1, 8)), jnp.float32)
    weight_o = scatter_about(streams_of[7], (D, BW), BW ** -0.5, 0.125, ((0, 16), (1, 8)), jnp.float32)
    first_q = scatter_about(streams_of[8], (RANK, QUERY_COLUMNS), 1.0, 6.0, ((0, 16), (1, 8)), jnp.float32)
    second_q = jnp.clip(jnp.exp(math.log(4.0) - 2.7725887 * jax.random.uniform(streams_of[9], (RANK, QUERY_COLUMNS), jnp.float32) ** steps_of(streams_of[9], (RANK, QUERY_COLUMNS), ((0, 16), (1, 8)), -0.2, 0.2)), 0.25, 4.0)
    first_o = scatter_about(streams_of[10], (RANK, BW), 1.0, 6.0, ((0, 16), (1, 8)), jnp.float32)
    second_o = jnp.clip(jnp.exp(math.log(4.0) - 2.7725887 * jax.random.uniform(streams_of[11], (RANK, BW), jnp.float32) ** steps_of(streams_of[11], (RANK, BW), ((0, 16), (1, 8)), -0.2, 0.2)), 0.25, 4.0)
    return dict(query_latent_rows=query_latent_rows, grad_q=grad_q, head_out=head_out, grad_out=grad_out, proj_q=proj_q, proj_o=proj_o, query_up_weight=query_up_weight, weight_o=weight_o, first_q=first_q, second_q=second_q, first_o=first_o, second_o=second_o)


beta_first = 0.8
beta_second = 0.9
epsilon = 1e-08
decay_rate = 2.0
step_rate = 0.05

def moments(first, second, reduced, clip_scale):
    scaled = clip_scale * reduced
    first_new = beta_first * first + (1.0 - beta_first) * scaled
    second_new = beta_second * second + (1.0 - beta_second) * scaled * scaled
    return (first_new, second_new, first_new / (jnp.sqrt(second_new) + epsilon))

def reference(query_latent_rows, grad_q, head_out, grad_out, proj_q, proj_o, query_up_weight, weight_o, first_q, second_q, first_o, second_o):
    highest = lax.Precision.HIGHEST
    grad_full_q = jnp.dot(query_latent_rows.T, grad_q, preferred_element_type=jnp.float32)
    grad_full_o = jnp.dot(grad_out.T, head_out, preferred_element_type=jnp.float32)
    basis_q = proj_q.astype(jnp.float32)
    basis_o = proj_o.astype(jnp.float32)
    low_q = jnp.dot(basis_q.T, grad_full_q, precision=highest, preferred_element_type=jnp.float32)
    low_o = jnp.dot(basis_o.T, grad_full_o, precision=highest, preferred_element_type=jnp.float32)
    sum_squares = jnp.sum(low_q * low_q) + jnp.sum(low_o * low_o)
    target = math.sqrt(RANK * (QUERY_COLUMNS + BW))
    clip_scale = jnp.minimum(1.0, target / jnp.sqrt(sum_squares))
    first_nq, second_nq, direct_q = moments(first_q, second_q, low_q, clip_scale)
    first_no, second_no, direct_o = moments(first_o, second_o, low_o, clip_scale)
    step_q = jnp.dot(basis_q, direct_q, precision=highest, preferred_element_type=jnp.float32) + decay_rate * query_up_weight
    step_o = jnp.dot(basis_o, direct_o, precision=highest, preferred_element_type=jnp.float32) + decay_rate * weight_o
    new_weight_q = query_up_weight - step_rate * step_q
    new_weight_o = weight_o - step_rate * step_o
    return (new_weight_q, new_weight_o, first_nq, second_nq, first_no, second_no, step_q, step_o, new_weight_q.astype(jnp.bfloat16), new_weight_o.astype(jnp.bfloat16))
```

```python
import math

import jax
import jax.numpy as jnp
from jax import lax
from jax.experimental import pallas as pl
from jax.experimental.pallas import tpu as pltpu
from jax.sharding import PartitionSpec as P

FS, TP = "fs", "tp"
SIDE = 4
N_FS, N_TP = 16, 8

beta_first = 0.8
beta_second = 0.9
epsilon = 1e-08
decay_rate = 2.0
step_rate = 0.05

BF16, F32 = jnp.bfloat16, jnp.float32


def dot(a, b):
    return lax.dot_general(a, b, (((1,), (0,)), ((), ())), preferred_element_type=F32)


def dot_t(a, b):
    return lax.dot_general(a, b, (((0,), (0,)), ((), ())), preferred_element_type=F32)


class PlaneGather:
    def __init__(self, ref_of, rows, ssem, rsem, a, b, fs_of):
        self.ref_of, self.rows, self.ss, self.rs = ref_of, rows, ssem, rsem
        self.a, self.b, self.fs_of = a, b, fs_of
        self.am = [a, (a + 3) % SIDE, (a + 1) % SIDE, (a + 2) % SIDE]
        self.bp, self.bm, self.b2 = (b + 1) % SIDE, (b + 3) % SIDE, (b + 2) % SIDE
        self.sent = []

    def part(self, half):
        h = self.rows // 2
        return {None: (0, self.rows), 0: (0, h), 1: (h, h)}[half]

    def copy(self, j, block, half, to):
        lo, n = self.part(half)
        ref = self.ref_of(block, lo, n)
        return pltpu.make_async_remote_copy(
            src_ref=ref, dst_ref=ref, send_sem=self.ss.at[j], recv_sem=self.rs.at[j],
            device_id={FS: to}, device_id_type=pl.DeviceIdType.MESH)

    def send(self, j, block, half, to):
        c = self.copy(j, block, half, to)
        c.start()
        self.sent.append(c)

    def got(self, j, block, half):
        self.copy(j, block, half, block).wait_recv()

    def along_b(self, m):
        blk = self.fs_of(self.am[m], self.b)
        self.send(4 + 2 * m, blk, None, self.fs_of(self.a, self.bp))
        self.send(5 + 2 * m, blk, None, self.fs_of(self.a, self.bm))

    def start(self):
        own = self.fs_of(self.a, self.b)
        self.send(0, own, None, self.fs_of(self.am[2], self.b))
        self.send(1, own, None, self.fs_of(self.am[1], self.b))
        self.along_b(0)
        return own

    def take_a(self, m):
        blk = self.fs_of(self.am[m], self.b)
        self.got(m - 1, blk, None)
        self.send(m + 1, blk, m - 1, self.fs_of(self.am[3 - m], self.b))
        self.along_b(m)
        return blk

    def take_a2(self):
        blk = self.fs_of(self.am[3], self.b)
        self.got(2, blk, 0)
        self.got(3, blk, 1)
        self.along_b(3)
        return blk

    def take_b(self, m):
        lo = self.fs_of(self.am[m], self.bm)
        self.got(4 + 2 * m, lo, None)
        self.send(12 + 2 * m, lo, 0, self.fs_of(self.a, self.bp))
        hi = self.fs_of(self.am[m], self.bp)
        self.got(5 + 2 * m, hi, None)
        self.send(13 + 2 * m, hi, 1, self.fs_of(self.a, self.bm))
        return lo, hi

    def take_b2(self, m):
        blk = self.fs_of(self.am[m], self.b2)
        self.got(12 + 2 * m, blk, 0)
        self.got(13 + 2 * m, blk, 1)
        return blk

    def finish(self):
        for c in self.sent:
            c.wait_send()


def moments(first, second, reduced, clip_scale):
    scaled = clip_scale * reduced
    first_new = beta_first * first + (1.0 - beta_first) * scaled
    second_new = beta_second * second + (1.0 - beta_second) * scaled * scaled
    return first_new, second_new, first_new / (jnp.sqrt(second_new) + epsilon)


def exchange_kernel(target, xq_h, gq_h, ho_h, go_h, pq_h, po_h, wq_h, wo_h, fq_h, sq_h, fo_h, so_h,
                    pf, pw, dirs, low, scale,
                    xq, gq, ho, go, wq, wo, fq, sq, fo, so, zq, zo, rs_out, rs_in, sum_tp, sum_fs,
                    in_sem, p_ss, p_rs, w_ss, w_rs, sib_ss, sib_rs, rs_ss, rs_rs, st_ss, st_rs, sf_ss, sf_rs,
                    ag_ss, ag_rs):
    i, t = lax.axis_index(FS), lax.axis_index(TP)
    z, y, c = i // SIDE, i % SIDE, t % 2
    a, b = y * (1 - c) + z * c, z * (1 - c) + y * c

    def fs_of(a_, b_):
        return a_ * (1 + 3 * c) + b_ * (4 - 3 * c)

    nq, no = pq_h.shape[0], po_h.shape[0]
    own_p = pf.at[i]
    loads = []

    def load(src, dst):
        cp = pltpu.make_async_copy(src, dst, in_sem.at[len(loads)])
        cp.start()
        loads.append(cp)
        return cp

    half = (nq + no) // 2
    p1 = load(pq_h, pf.at[i, 0, pl.ds(0, nq)])
    p2 = load(po_h.at[pl.ds(0, half - nq)], pf.at[i, 0, pl.ds(nq, half - nq)])
    p3 = load(po_h.at[pl.ds(half - nq, half)], pf.at[i, 1])
    w1, w2 = load(wq_h, wq), load(wo_h, wo)
    big = [load(go_h, go), load(xq_h, xq), load(gq_h, gq), load(ho_h, ho)]
    small = [load(s, d) for s, d in ((fq_h, fq), (sq_h, sq), (fo_h, fo), (so_h, so))]

    barrier = pltpu.get_barrier_semaphore()
    nbrs = [{FS: fs_of((a + 1) % SIDE, b)}, {FS: fs_of((a + 3) % SIDE, b)},
            {FS: fs_of(a, (b + 1) % SIDE)}, {FS: fs_of(a, (b + 3) % SIDE)}]
    nbrs += [{TP: (t + d) % N_TP} for d in range(1, N_TP)]
    for n in nbrs:
        pl.semaphore_signal(barrier, inc=1, device_id=n, device_id_type=pl.DeviceIdType.MESH)
    p1.wait()
    p2.wait()
    p3.wait()
    pl.semaphore_wait(barrier, len(nbrs))

    pg = PlaneGather(lambda blk, lo, n: pf.at[blk, c, pl.ds(lo, n)], half, p_ss, p_rs, a, b, fs_of)
    sib = {TP: t + 1 - 2 * c}
    sib_sent = []

    def sib_copy(blk, which):
        ref = pf.at[blk, which]
        return pltpu.make_async_remote_copy(
            src_ref=ref, dst_ref=ref, send_sem=sib_ss.at[blk], recv_sem=sib_rs.at[blk],
            device_id=sib, device_id_type=pl.DeviceIdType.MESH)

    def to_sib(blk):
        cp = sib_copy(blk, c)
        cp.start()
        sib_sent.append(cp)

    pg.start()

    w1.wait()
    w2.wait()
    row = 0
    for src in (wq, wo):
        for col in range(0, src.shape[1], 128):
            pw[i, row:row + src.shape[0], :] = src[:, col:col + 128].astype(BF16)
            row += src.shape[0]

    to_sib(pg.take_a(1))
    to_sib(pg.take_a(2))
    for blk in pg.take_b(0):
        to_sib(blk)
    to_sib(pg.take_a2())
    for m in (1, 2, 3):
        for blk in pg.take_b(m):
            to_sib(blk)
    for m in range(4):
        to_sib(pg.take_b2(m))

    def wait_sib(k, _):
        blk = (i + k) % N_FS
        sib_copy(blk, 1 - c).wait_recv()
        return 0

    lax.fori_loop(1, N_FS, wait_sib, 0)
    for cp in big:
        cp.wait()

    tile = 256

    def project(m, _):
        rows = pl.ds(m * tile, tile)
        whole = pf[...].reshape(N_FS, 2 * half, pf.shape[3])
        zo[rows, :] = dot(go[rows, :], whole[:, nq:, :].reshape(N_FS * no, -1)).astype(BF16)
        zq[rows, :] = dot(xq[rows, :], whole[:, :nq, :].reshape(N_FS * nq, -1)).astype(BF16)
        return 0

    lax.fori_loop(0, xq.shape[0] // tile, project, 0)
    part = jnp.concatenate([dot_t(zq[...], gq[...]), dot_t(zo[...], ho[...])], axis=1)
    rs_out[...] = part.astype(BF16).reshape(rs_out.shape)

    def rs_copy(d):
        return pltpu.make_async_remote_copy(
            src_ref=rs_out.at[(i + d) % N_FS], dst_ref=rs_in.at[d], send_sem=rs_ss.at[d], recv_sem=rs_rs,
            device_id={FS: (i + d) % N_FS}, device_id_type=pl.DeviceIdType.MESH)

    def start(make):
        def body(d, _):
            make(d).start()
            return 0
        return body

    def wait_send(make):
        def body(d, _):
            make(d).wait_send()
            return 0
        return body

    lax.fori_loop(1, N_FS, start(rs_copy), 0)

    wg = PlaneGather(lambda blk, lo, n: pw.at[blk, pl.ds(lo, n)], pw.shape[1], w_ss, w_rs, a, b, fs_of)
    wg.start()

    arrived = rs_in.at[pl.ds(1, N_FS - 1)]
    pltpu.make_async_copy(arrived, arrived, rs_rs).wait()
    reduced = rs_out[i].astype(F32)
    for d in range(1, N_FS):
        reduced = reduced + rs_in[d].astype(F32)
    low[...] = reduced
    local = jnp.sum(jnp.sum(reduced * reduced, axis=1, keepdims=True), axis=0, keepdims=True)
    sum_tp[0] = jnp.broadcast_to(local, sum_tp.shape[1:])

    def st_copy(d):
        return pltpu.make_async_remote_copy(
            src_ref=sum_tp.at[0], dst_ref=sum_tp.at[d], send_sem=st_ss.at[d], recv_sem=st_rs,
            device_id={TP: (t + d) % N_TP}, device_id_type=pl.DeviceIdType.MESH)

    lax.fori_loop(1, N_TP, start(st_copy), 0)
    wg.take_a(1)
    wg.take_a(2)
    rest = sum_tp.at[pl.ds(1, N_TP - 1)]
    pltpu.make_async_copy(rest, rest, st_rs).wait()
    sum_fs[0] = jnp.sum(sum_tp[...], axis=0)

    def sf_copy(d):
        return pltpu.make_async_remote_copy(
            src_ref=sum_fs.at[0], dst_ref=sum_fs.at[d], send_sem=sf_ss.at[d], recv_sem=sf_rs,
            device_id={FS: (i + d) % N_FS}, device_id_type=pl.DeviceIdType.MESH)

    lax.fori_loop(1, N_FS, start(sf_copy), 0)
    wg.take_b(0)
    wg.take_a2()
    rest = sum_fs.at[pl.ds(1, N_FS - 1)]
    pltpu.make_async_copy(rest, rest, sf_rs).wait()
    total = jnp.sum(sum_fs[...], axis=0)
    clip = jnp.minimum(1.0, target / jnp.sqrt(total))
    scale[...] = clip
    for cp in small:
        cp.wait()
    s = clip[0:1, 0:1]
    cq = fq.shape[1]
    _, _, dq = moments(fq[...], sq[...], low[:, :cq], s)
    _, _, do = moments(fo[...], so[...], low[:, cq:], s)
    dirs[i] = jnp.concatenate([dq, do], axis=1).astype(BF16)

    def ag_copy(d):
        return pltpu.make_async_remote_copy(
            src_ref=dirs.at[i], dst_ref=dirs.at[i], send_sem=ag_ss.at[d], recv_sem=ag_rs.at[d],
            device_id={FS: (i + d) % N_FS}, device_id_type=pl.DeviceIdType.MESH)

    lax.fori_loop(1, N_FS, start(ag_copy), 0)
    for m in (1, 2, 3):
        wg.take_b(m)
    for m in range(4):
        wg.take_b2(m)

    def ag_wait(d, _):
        blk = (i - d + N_FS) % N_FS
        pltpu.make_async_remote_copy(
            src_ref=dirs.at[blk], dst_ref=dirs.at[blk], send_sem=ag_ss.at[d], recv_sem=ag_rs.at[d],
            device_id={FS: blk}, device_id_type=pl.DeviceIdType.MESH).wait_recv()
        return 0

    lax.fori_loop(1, N_FS, ag_wait, 0)
    pg.finish()
    wg.finish()
    for cp in sib_sent:
        cp.wait_send()
    lax.fori_loop(1, N_FS, wait_send(rs_copy), 0)
    lax.fori_loop(1, N_TP, wait_send(st_copy), 0)
    lax.fori_loop(1, N_FS, wait_send(sf_copy), 0)
    lax.fori_loop(1, N_FS, wait_send(ag_copy), 0)


def update_kernel(pf, pw, dirs, low, scale, pq, po, wq, wo, fq, sq, fo, so,
                  nwq, nwo, nfq, nsq, nfo, nso, stq, sto, cpq, cpo):
    cq, co = fq.shape[1], fo.shape[1]
    nq, no = pq.shape[0], po.shape[0]
    d = dirs[...].reshape(-1, cq + co)
    dq, do = d[:, :cq], d[:, cq:]
    n = pf.shape[0]
    whole = pf[...].reshape(n, nq + no, pf.shape[3])
    mq = dot(whole[:, :nq, :].reshape(n * nq, -1), dq)
    mo = dot(whole[:, nq:, :].reshape(n * no, -1), do)
    keep = 1.0 - step_rate * decay_rate
    for col in range(0, cq, 128):
        w = pw[:, (col // 128) * nq:(col // 128 + 1) * nq, :].astype(F32).reshape(n * nq, 128)
        cpq[:, col:col + 128] = (keep * w - step_rate * mq[:, col:col + 128]).astype(BF16)
    base = (cq // 128) * nq
    for col in range(0, co, 128):
        at = base + (col // 128) * no
        w = pw[:, at:at + no, :].astype(F32).reshape(n * no, 128)
        cpo[:, col:col + 128] = (keep * w - step_rate * mo[:, col:col + 128]).astype(BF16)

    @pl.when(pl.program_id(0) == 0)
    def _():
        s = scale[0:1, 0:1]
        f, v, _ = moments(fq[...], sq[...], low[:, :cq], s)
        nfq[...] = f
        nsq[...] = v
        f, v, _ = moments(fo[...], so[...], low[:, cq:], s)
        nfo[...] = f
        nso[...] = v
        for p_, d_, w_, st_, nw_ in ((pq, dq, wq, stq, nwq), (po, do, wo, sto, nwo)):
            step = dot(p_[...], d_) + decay_rate * w_[...]
            st_[...] = step
            nw_[...] = w_[...] - step_rate * step


def per_device(query_latent_rows, grad_q, head_out, grad_out, proj_q, proj_o, query_up_weight, weight_o,
               first_q, second_q, first_o, second_o):
    nq, no, rank = proj_q.shape[0], proj_o.shape[0], proj_q.shape[1]
    cq, co = first_q.shape[1], first_o.shape[1]
    rows = first_q.shape[0]
    target = math.sqrt(rows * N_FS * (cq + co) * N_TP)
    half = (nq + no) // 2
    wrows = (nq * cq + no * co) // 128
    sds = jax.ShapeDtypeStruct
    any_ = pl.BlockSpec(memory_space=pl.ANY)
    vmem = pl.BlockSpec(memory_space=pltpu.VMEM)
    dma = pltpu.SemaphoreType.DMA
    V = pltpu.VMEM
    ins = (query_latent_rows, grad_q, head_out, grad_out, proj_q, proj_o, query_up_weight, weight_o,
           first_q, second_q, first_o, second_o)
    like = lambda x: V(x.shape, x.dtype)
    tokens = query_latent_rows.shape[0]

    def ex(*refs):
        exchange_kernel(target, *refs)

    pf, pw, dirs, low, scale = pl.pallas_call(
        ex,
        out_shape=[sds((N_FS, 2, half, rank), BF16), sds((N_FS, wrows, 128), BF16),
                   sds((N_FS, rows, cq + co), BF16), sds((rows, cq + co), F32), sds((8, 128), F32)],
        in_specs=[any_] * len(ins),
        out_specs=[vmem] * 5,
        scratch_shapes=[
            like(query_latent_rows), like(grad_q), like(head_out), like(grad_out),
            like(query_up_weight), like(weight_o), like(first_q), like(second_q), like(first_o), like(second_o),
            V((tokens, rank), BF16), V((tokens, rank), BF16),
            V((N_FS, rows, cq + co), BF16), V((N_FS, rows, cq + co), BF16),
            V((N_TP, 8, 128), F32), V((N_FS, 8, 128), F32),
            dma((13,)), dma((20,)), dma((20,)), dma((20,)), dma((20,)), dma((N_FS,)), dma((N_FS,)),
            dma((N_FS,)), dma, dma((N_TP,)), dma, dma((N_FS,)), dma, dma((N_FS,)), dma((N_FS,)),
        ],
        compiler_params=pltpu.CompilerParams(collective_id=0, has_side_effects=True,
                                             vmem_limit_bytes=48 * 1024 * 1024),
        name="exchange",
    )(*ins)

    G = 4
    n = N_FS // G
    full = lambda x: pl.BlockSpec(x.shape, lambda g: (0,) * len(x.shape))
    outs = [sds((nq, cq), F32), sds((no, co), F32), sds((rows, cq), F32), sds((rows, cq), F32),
            sds((rows, co), F32), sds((rows, co), F32), sds((nq, cq), F32), sds((no, co), F32)]
    tail = (proj_q, proj_o, query_up_weight, weight_o, first_q, second_q, first_o, second_o)
    return tuple(pl.pallas_call(
        update_kernel,
        grid=(G,),
        in_specs=[pl.BlockSpec((n, 2, half, rank), lambda g: (g, 0, 0, 0)),
                  pl.BlockSpec((n, wrows, 128), lambda g: (g, 0, 0)),
                  full(dirs), full(low), full(scale)] + [full(x) for x in tail],
        out_specs=[full(o) for o in outs] + [pl.BlockSpec((n * nq, cq), lambda g: (g, 0)),
                                             pl.BlockSpec((n * no, co), lambda g: (g, 0))],
        out_shape=outs + [sds((N_FS * nq, cq), BF16), sds((N_FS * no, co), BF16)],
        compiler_params=pltpu.CompilerParams(vmem_limit_bytes=24 * 1024 * 1024),
        name="update",
    )(pf, pw, dirs, low, scale, *tail))


def solution(mesh):
    rows, both, cols = P(FS, None), P(FS, TP), P(None, TP)
    return jax.shard_map(
        per_device,
        mesh=mesh,
        in_specs=(rows, both, both, rows, rows, rows) + (both,) * 6,
        out_specs=(both,) * 8 + (cols, cols),
        check_vma=False,
    )
```

```python
import math

import jax
import jax.numpy as jnp
from jax import lax
from jax.experimental import pallas as pl
from jax.experimental.pallas import tpu as pltpu
from jax.sharding import PartitionSpec as P

FS, TP = "fs", "tp"
SIDE = 4
N_FS, N_TP = 16, 8

beta_first = 0.8
beta_second = 0.9
epsilon = 1e-08
decay_rate = 2.0
step_rate = 0.05

BF16, F32 = jnp.bfloat16, jnp.float32

NP, NW = 2, 3
PLAN = {
    "0": [(0, 0)],
    "1": [(1, 0)],
    "2": [(0, 1), (2, 0)],
    "3": [(0, 2), (1, 1)],
    "4": [(0, 3), (0, 4), (1, 2), (2, 1)],
    "5": [(0, 5), (1, 3), (1, 4), (2, 2)],
    "6": [(1, 5), (2, 3), (2, 4)],
    "7": [(2, 5)],
}


def dot(a, b):
    return lax.dot_general(a, b, (((1,), (0,)), ((), ())), preferred_element_type=F32)


def dot_t(a, b):
    return lax.dot_general(a, b, (((0,), (0,)), ((), ())), preferred_element_type=F32)


class PlaneGather:
    def __init__(self, ref_of, rows, ssem, rsem, a, b, fs_of, direct=False):
        self.direct = direct
        self.ref_of, self.rows, self.ss, self.rs = ref_of, rows, ssem, rsem
        self.a, self.b, self.fs_of = a, b, fs_of
        self.am = [a, (a + 3) % SIDE, (a + 1) % SIDE, (a + 2) % SIDE]
        self.bp, self.bm, self.b2 = (b + 1) % SIDE, (b + 3) % SIDE, (b + 2) % SIDE
        self.sent = []

    def part(self, half):
        h = self.rows // 2
        return {None: (0, self.rows), 0: (0, h), 1: (h, h)}[half]

    def copy(self, j, block, half, to):
        lo, n = self.part(half)
        ref = self.ref_of(block, lo, n)
        return pltpu.make_async_remote_copy(
            src_ref=ref, dst_ref=ref, send_sem=self.ss.at[j], recv_sem=self.rs.at[j],
            device_id={FS: to}, device_id_type=pl.DeviceIdType.MESH)

    def send(self, j, block, half, to):
        c = self.copy(j, block, half, to)
        c.start()
        self.sent.append(c)

    def got(self, j, block, half):
        self.copy(j, block, half, block).wait_recv()

    def along_b(self, m):
        blk = self.fs_of(self.am[m], self.b)
        self.send(4 + 2 * m, blk, None, self.fs_of(self.a, self.bp))
        self.send(5 + 2 * m, blk, None, self.fs_of(self.a, self.bm))

    def start(self):
        own = self.fs_of(self.a, self.b)
        self.send(0, own, None, self.fs_of(self.am[2], self.b))
        self.send(1, own, None, self.fs_of(self.am[1], self.b))
        if self.direct:
            self.send(2, own, None, self.fs_of(self.am[3], self.b))
        self.along_b(0)
        return own

    def take_a(self, m):
        blk = self.fs_of(self.am[m], self.b)
        self.got(m - 1, blk, None)
        if not self.direct:
            self.send(m + 1, blk, m - 1, self.fs_of(self.am[3 - m], self.b))
        self.along_b(m)
        return blk

    def take_a2(self):
        blk = self.fs_of(self.am[3], self.b)
        if self.direct:
            self.got(2, blk, None)
        else:
            self.got(2, blk, 0)
            self.got(3, blk, 1)
        self.along_b(3)
        return blk

    def take_b(self, m):
        lo = self.fs_of(self.am[m], self.bm)
        self.got(4 + 2 * m, lo, None)
        self.send(12 + 2 * m, lo, 0, self.fs_of(self.a, self.bp))
        hi = self.fs_of(self.am[m], self.bp)
        self.got(5 + 2 * m, hi, None)
        self.send(13 + 2 * m, hi, 1, self.fs_of(self.a, self.bm))
        return lo, hi

    def take_b2(self, m):
        blk = self.fs_of(self.am[m], self.b2)
        self.got(12 + 2 * m, blk, 0)
        self.got(13 + 2 * m, blk, 1)
        return blk

    def finish(self):
        for c in self.sent:
            c.wait_send()


def moments(first, second, reduced, clip_scale):
    scaled = clip_scale * reduced
    first_new = beta_first * first + (1.0 - beta_first) * scaled
    second_new = beta_second * second + (1.0 - beta_second) * scaled * scaled
    return first_new, second_new, first_new / (jnp.sqrt(second_new) + epsilon)


def exchange_kernel(target, xq_h, gq_h, ho_h, go_h, pq_h, po_h, wq_h, wo_h, fq_h, sq_h, fo_h, so_h,
                    pf, pw, lowg, low, scale,
                    xq, gq, ho, go, wq, wo, fq, sq, fo, so, ho_t, gq_t, grad_o, grad_q, acc, rs_out, rs_in,
                    sum_tp, sum_fs,
                    in_sem, p_ss, p_rs, w_ss, w_rs, sib_ss, sib_rs, rs_ss, rs_rs,
                    st_ss, st_rs, sf_ss, sf_rs, ag_ss, ag_rs):
    i, t = lax.axis_index(FS), lax.axis_index(TP)
    z, y, c = i // SIDE, i % SIDE, t % 2
    a, b = y * (1 - c) + z * c, z * (1 - c) + y * c

    def fs_of(a_, b_):
        return a_ * (1 + 3 * c) + b_ * (4 - 3 * c)

    nq, no = pq_h.shape[0], po_h.shape[0]
    loads = []

    def load(src, dst):
        cp = pltpu.make_async_copy(src, dst, in_sem.at[len(loads)])
        cp.start()
        loads.append(cp)
        return cp

    half = (nq + no) // 2
    p1 = load(pq_h, pf.at[i, 0, pl.ds(0, nq)])
    p2 = load(po_h.at[pl.ds(0, half - nq)], pf.at[i, 0, pl.ds(nq, half - nq)])
    p3 = load(po_h.at[pl.ds(half - nq, half)], pf.at[i, 1])
    own_f32 = [load(s, d) for s, d in ((wq_h, wq), (wo_h, wo), (fq_h, fq), (fo_h, fo), (sq_h, sq), (so_h, so))]
    l_ho, l_gq = load(ho_h, ho), load(gq_h, gq)
    step = go.shape[1] // 4
    l_go = [load(go_h.at[:, pl.ds(k * step, step)], go.at[:, pl.ds(k * step, step)]) for k in range(4)]
    l_xq = load(xq_h, xq)

    barrier = pltpu.get_barrier_semaphore()
    nbrs = [{FS: fs_of((a + d) % SIDE, b)} for d in (1, 2, 3)] + [
        {FS: fs_of(a, (b + d) % SIDE)} for d in (1, 2, 3)]
    nbrs += [{TP: (t + d) % N_TP} for d in range(1, N_TP)]
    for n in nbrs:
        pl.semaphore_signal(barrier, inc=1, device_id=n, device_id_type=pl.DeviceIdType.MESH)
    for cp in (p1, p2, p3):
        cp.wait()
    pl.semaphore_wait(barrier, len(nbrs))

    piece = half // NP
    pgs = [PlaneGather(lambda blk, lo, n, g=g: pf.at[blk, c, pl.ds(g * piece + lo, n)], piece,
                       p_ss.at[g], p_rs.at[g], a, b, fs_of, direct=True) for g in range(NP)]
    wpiece = pw.shape[1] // NW
    wgs = [PlaneGather(lambda blk, lo, n, g=g: pw.at[blk, pl.ds(g * wpiece + lo, n)], wpiece,
                       w_ss.at[g], w_rs.at[g], a, b, fs_of) for g in range(NW)]
    sib = {TP: t + 1 - 2 * c}
    sib_sent = []

    def sib_copy(g, blk, which):
        ref = pf.at[blk, which, pl.ds(g * piece, piece)]
        return pltpu.make_async_remote_copy(
            src_ref=ref, dst_ref=ref, send_sem=sib_ss.at[g, blk], recv_sem=sib_rs.at[g, blk],
            device_id=sib, device_id_type=pl.DeviceIdType.MESH)

    def to_sib(g, *blks):
        for blk in blks:
            cp = sib_copy(g, blk, c)
            cp.start()
            sib_sent.append(cp)

    for g in pgs:
        g.start()

    for cp in own_f32:
        cp.wait()
    row = 0
    for src in (wq, wo, fq, fo, sq, so):
        for col in range(0, src.shape[1], 128):
            part = src[:, col:col + 128]
            if src is wq or src is wo:
                part = part * (1.0 - step_rate * decay_rate)
            pw[i, row:row + src.shape[0], :] = part.astype(BF16)
            row += src.shape[0]

    def w_stage(w, s):
        g = wgs[w]
        if s == 0:
            g.start()
        elif s == 1:
            g.take_a(1)
            g.take_a(2)
        elif s == 2:
            g.take_b(0)
            g.take_a2()
        elif s == 3:
            g.take_b(1)
            g.take_b(2)
        elif s == 4:
            g.take_b(3)
        else:
            for m in range(4):
                g.take_b2(m)

    def fill(slot):
        for w, s in PLAN.get(slot, ()):
            w_stage(w, s)

    def gradient_o(k):
        l_go[k].wait()
        for at in range(k * step, (k + 1) * step, 256):
            grad_o[:, at:at + 256] = dot(ho_t[...], go[:, at:at + 256]).astype(BF16)

    def gradient_q(k):
        for at in range(k * 512, (k + 1) * 512, 256):
            grad_q[:, at:at + 256] = dot(gq_t[...], xq[:, at:at + 256]).astype(BF16)

    def wait_sib(*blks):
        for blk in blks:
            for g in range(NP):
                sib_copy(g, blk, 1 - c).wait_recv()

    def project_o(*blks):
        out = None
        for blk in blks:
            p = pf[blk].reshape(2 * half, -1)[nq:]
            d = dot(grad_o[:, pl.ds(pl.multiple_of(blk * no, no), no)], p)
            out = d if out is None else out + d
        return out

    a1, a2, a3 = (a + 3) % SIDE, (a + 1) % SIDE, (a + 2) % SIDE
    b1, b2, b3 = (b + 3) % SIDE, (b + 1) % SIDE, (b + 2) % SIDE
    fill("0")
    l_ho.wait()
    ho_t[...] = ho[...].T
    for g, pg in enumerate(pgs):
        to_sib(g, pg.take_a(1))
        to_sib(g, pg.take_a(2))
    fill("1")
    l_gq.wait()
    gq_t[...] = gq[...].T
    gradient_o(0)
    for g, pg in enumerate(pgs):
        to_sib(g, *pg.take_b(0))
        to_sib(g, pg.take_a2())
    fill("2")
    gradient_o(1)
    for g, pg in enumerate(pgs):
        to_sib(g, *pg.take_b(1))
        to_sib(g, *pg.take_b(2))
    fill("3")
    gradient_o(2)
    for g, pg in enumerate(pgs):
        to_sib(g, *pg.take_b(3))
    fill("4")
    gradient_o(3)
    for g, pg in enumerate(pgs):
        to_sib(g, pg.take_b2(0))
    l_xq.wait()
    gradient_q(0)
    for g, pg in enumerate(pgs):
        to_sib(g, pg.take_b2(1))
        to_sib(g, pg.take_b2(2))
    gradient_q(1)
    near = [fs_of(p, q) for p in (a1, a2) for q in (b1, b2)] + [fs_of(a, b1), fs_of(a, b2), fs_of(a1, b), fs_of(a2, b)]
    wait_sib(*near)
    acc[...] = project_o(i, *near)
    for g, pg in enumerate(pgs):
        to_sib(g, pg.take_b2(3))
    fill("5")
    far = [fs_of(a3, b), fs_of(a, b3), fs_of(a3, b1), fs_of(a3, b2), fs_of(a1, b3), fs_of(a2, b3), fs_of(a3, b3)]
    wait_sib(*far)
    part_o = acc[...] + project_o(*far)
    part_q = dot(grad_q[...], pf[:, 0, 0:nq, :].reshape(N_FS * nq, -1))
    cq = fq.shape[1]
    rs_out[:, :, cq:] = part_o.T.astype(BF16).reshape(N_FS, -1, part_o.shape[0])
    rs_out[:, :, :cq] = part_q.T.astype(BF16).reshape(N_FS, -1, part_q.shape[0])

    def rs_copy(d):
        return pltpu.make_async_remote_copy(
            src_ref=rs_out.at[(i + d) % N_FS], dst_ref=rs_in.at[d], send_sem=rs_ss.at[d], recv_sem=rs_rs,
            device_id={FS: (i + d) % N_FS}, device_id_type=pl.DeviceIdType.MESH)

    def start(make):
        def body(d, _):
            make(d).start()
            return 0
        return body

    def wait_send(make):
        def body(d, _):
            make(d).wait_send()
            return 0
        return body

    lax.fori_loop(1, N_FS, start(rs_copy), 0)
    fill("6")
    arrived = rs_in.at[pl.ds(1, N_FS - 1)]
    pltpu.make_async_copy(arrived, arrived, rs_rs).wait()
    reduced = rs_out[i].astype(F32)
    for d in range(1, N_FS):
        reduced = reduced + rs_in[d].astype(F32)
    low[...] = reduced
    lowg[i] = reduced.astype(BF16)
    sum_tp[t] = jnp.full(sum_tp.shape[1:], jnp.sum(reduced * reduced), F32)

    def st_copy(d, src=None):
        return pltpu.make_async_remote_copy(
            src_ref=sum_tp.at[t], dst_ref=sum_tp.at[t], send_sem=st_ss.at[d], recv_sem=st_rs.at[d],
            device_id={TP: (t + d) % N_TP}, device_id_type=pl.DeviceIdType.MESH)

    def sf_copy(d):
        return pltpu.make_async_remote_copy(
            src_ref=sum_fs.at[i], dst_ref=sum_fs.at[i], send_sem=sf_ss.at[d], recv_sem=sf_rs.at[d],
            device_id={FS: (i + d) % N_FS}, device_id_type=pl.DeviceIdType.MESH)

    def ag_copy(d):
        return pltpu.make_async_remote_copy(
            src_ref=lowg.at[i], dst_ref=lowg.at[i], send_sem=ag_ss.at[d], recv_sem=ag_rs.at[d],
            device_id={FS: (i + d) % N_FS}, device_id_type=pl.DeviceIdType.MESH)

    def arrivals(buf, me, n, axis, sems):
        def body(d, _):
            blk = (me - d + n) % n
            pltpu.make_async_remote_copy(
                src_ref=buf.at[blk], dst_ref=buf.at[blk], send_sem=sems.at[d], recv_sem=sems.at[d],
                device_id={axis: blk}, device_id_type=pl.DeviceIdType.MESH).wait_recv()
            return 0
        lax.fori_loop(1, n, body, 0)

    lax.fori_loop(1, N_TP, start(st_copy), 0)
    lax.fori_loop(1, N_FS, start(ag_copy), 0)
    fill("7")
    arrivals(sum_tp, t, N_TP, TP, st_rs)
    sum_fs[i] = jnp.sum(sum_tp[...], axis=0)
    lax.fori_loop(1, N_FS, start(sf_copy), 0)
    fill("8")
    arrivals(lowg, i, N_FS, FS, ag_rs)
    fill("9")
    arrivals(sum_fs, i, N_FS, FS, sf_rs)
    scale[...] = jnp.minimum(1.0, target / jnp.sqrt(jnp.sum(sum_fs[...], axis=0)))
    for g in pgs + wgs:
        g.finish()
    for cp in sib_sent:
        cp.wait_send()
    lax.fori_loop(1, N_FS, wait_send(rs_copy), 0)
    lax.fori_loop(1, N_TP, wait_send(st_copy), 0)
    lax.fori_loop(1, N_FS, wait_send(sf_copy), 0)
    lax.fori_loop(1, N_FS, wait_send(ag_copy), 0)


def update_kernel(pf, pw, lowg, low, scale, pq, po, wq, wo, fq, sq, fo, so,
                  nwq, nwo, nfq, nsq, nfo, nso, stq, sto, cpq, cpo, dirs):
    cq, co = fq.shape[1], fo.shape[1]
    nq, no, rows = pq.shape[0], po.shape[0], fq.shape[0]
    g = pl.program_id(0)
    n = cpq.shape[0] // nq
    blocks = (cq + co) // 128
    at_o = (cq // 128) * nq
    at_f = at_o + (co // 128) * no
    s = scale[0:1, 0:1]

    @pl.when(g == 0)
    def _():
        for j in range(blocks):
            f = pw[:, at_f + j * rows:at_f + (j + 1) * rows, :].astype(F32)
            v = pw[:, at_f + (blocks + j) * rows:at_f + (blocks + j + 1) * rows, :].astype(F32)
            l = lowg[:, :, j * 128:(j + 1) * 128].astype(F32)
            d = moments(f, v, l, s)[2]
            dirs[:, j * 128:(j + 1) * 128] = (-step_rate * d).reshape(-1, 128).astype(BF16)

    dq, do = dirs[:, :cq], dirs[:, cq:]
    own = pl.ds(g * n, n)
    whole = pf[own].reshape(n, nq + no, pf.shape[3])
    mq = dot(whole[:, :nq, :].reshape(n * nq, -1), dq)
    mo = dot(whole[:, nq:, :].reshape(n * no, -1), do)
    for col in range(0, cq, 128):
        w = pw[own, (col // 128) * nq:(col // 128 + 1) * nq, :].astype(F32).reshape(n * nq, 128)
        cpq[:, col:col + 128] = (w + mq[:, col:col + 128]).astype(BF16)
    for col in range(0, co, 128):
        at = at_o + (col // 128) * no
        w = pw[own, at:at + no, :].astype(F32).reshape(n * no, 128)
        cpo[:, col:col + 128] = (w + mo[:, col:col + 128]).astype(BF16)

    @pl.when(g == 0)
    def _():
        f, v, _ = moments(fq[...], sq[...], low[:, :cq], s)
        nfq[...] = f
        nsq[...] = v
        f, v, _ = moments(fo[...], so[...], low[:, cq:], s)
        nfo[...] = f
        nso[...] = v
        for p_, d_, w_, st_, nw_ in ((pq, dq, wq, stq, nwq), (po, do, wo, sto, nwo)):
            step = dot(p_[...], d_) * (-1.0 / step_rate) + decay_rate * w_[...]
            st_[...] = step
            nw_[...] = w_[...] - step_rate * step


def per_device(query_latent_rows, grad_q, head_out, grad_out, proj_q, proj_o, query_up_weight, weight_o,
               first_q, second_q, first_o, second_o):
    nq, no, rank = proj_q.shape[0], proj_o.shape[0], proj_q.shape[1]
    cq, co = first_q.shape[1], first_o.shape[1]
    rows = first_q.shape[0]
    target = math.sqrt(rows * N_FS * (cq + co) * N_TP)
    half = (nq + no) // 2
    wrows = (nq * cq + no * co + 2 * rows * (cq + co)) // 128
    sds = jax.ShapeDtypeStruct
    dma = pltpu.SemaphoreType.DMA
    V = pltpu.VMEM
    ins = (query_latent_rows, grad_q, head_out, grad_out, proj_q, proj_o, query_up_weight, weight_o,
           first_q, second_q, first_o, second_o)
    like = lambda x: V(x.shape, x.dtype)
    tokens = query_latent_rows.shape[0]

    def ex(*refs):
        exchange_kernel(target, *refs)

    gathered = pl.pallas_call(
        ex,
        out_shape=[V((N_FS, 2, half, rank), BF16), V((N_FS, wrows, 128), BF16),
                   V((N_FS, rows, cq + co), BF16), V((rows, cq + co), F32), V((8, 128), F32)],
        in_specs=[pl.BlockSpec(memory_space=pltpu.HBM)] * len(ins),
        out_specs=[pl.BlockSpec(memory_space=pltpu.VMEM)] * 5,
        scratch_shapes=[
            like(query_latent_rows), like(grad_q), like(head_out), like(grad_out),
            like(query_up_weight), like(weight_o), like(first_q), like(second_q), like(first_o), like(second_o),
            V((co, tokens), BF16), V((cq, tokens), BF16), V((co, N_FS * no), BF16), V((cq, N_FS * nq), BF16),
            V((co, rank), F32), V((N_FS, rows, cq + co), BF16), V((N_FS, rows, cq + co), BF16),
            V((N_TP, 8, 128), F32), V((N_FS, 8, 128), F32),
            dma((16,)), dma((NP, 20)), dma((NP, 20)), dma((NW, 20)), dma((NW, 20)),
            dma((NP, N_FS)), dma((NP, N_FS)),
            dma((N_FS,)), dma, dma((N_TP,)), dma((N_TP,)),
            dma((N_FS,)), dma((N_FS,)), dma((N_FS,)), dma((N_FS,)),
        ],
        compiler_params=pltpu.CompilerParams(collective_id=0, has_side_effects=True,
                                             vmem_limit_bytes=48 * 1024 * 1024),
        name="exchange",
    )(*[pltpu.with_memory_space_constraint(x, pltpu.HBM) for x in ins])

    G = 4
    n = N_FS // G
    full = lambda x: pl.BlockSpec(x.shape, lambda g: (0,) * len(x.shape))
    outs = [sds((nq, cq), F32), sds((no, co), F32), sds((rows, cq), F32), sds((rows, cq), F32),
            sds((rows, co), F32), sds((rows, co), F32), sds((nq, cq), F32), sds((no, co), F32)]
    ops = (*gathered, proj_q, proj_o, query_up_weight, weight_o, first_q, second_q, first_o, second_o)
    return tuple(pl.pallas_call(
        update_kernel,
        grid=(G,),
        in_specs=[full(x) for x in ops],
        out_specs=[full(o) for o in outs] + [pl.BlockSpec((n * nq, cq), lambda g: (g, 0)),
                                             pl.BlockSpec((n * no, co), lambda g: (g, 0))],
        out_shape=outs + [sds((N_FS * nq, cq), BF16), sds((N_FS * no, co), BF16)],
        scratch_shapes=[V((rows * N_FS, cq + co), BF16)],
        compiler_params=pltpu.CompilerParams(vmem_limit_bytes=24 * 1024 * 1024),
        name="update",
    )(*ops))


def solution(mesh):
    rows, both, cols = P(FS, None), P(FS, TP), P(None, TP)
    return jax.shard_map(
        per_device,
        mesh=mesh,
        in_specs=(rows, both, both, rows, rows, rows) + (both,) * 6,
        out_specs=(both,) * 8 + (cols, cols),
        check_vma=False,
    )
```

```python
import math

import jax
import jax.numpy as jnp
from jax import lax
from jax.experimental import pallas as pl
from jax.experimental.pallas import tpu as pltpu
from jax.sharding import PartitionSpec as P

FS, TP = "fs", "tp"
SIDE = 4
N_FS, N_TP = 16, 8

beta_first = 0.8
beta_second = 0.9
epsilon = 1e-08
decay_rate = 2.0
step_rate = 0.05

BF16, F32 = jnp.bfloat16, jnp.float32

NP, NW = 1, 1
ORDER = [
    ("w", 0, 0), ("t",), ("g", 0), ("g", 1), ("g", 2),
    ("a", 1), ("a", 2), ("b", 0), ("g", 3), ("a", 3),
    ("g", 4), ("g", 5), ("g", 6), ("g", 7), ("b", 1), ("b", 2),
    ("g", 8), ("b", 3), ("g", 9), ("g", 10), ("g", 11),
    ("c", 0), ("w", 0, 1), ("g", 12), ("g", 13), ("g", 14), ("g", 15), ("c", 1), ("c", 2), ("q", 0), ("q", 1),
    ("q", 2), ("q", 3), ("near",), ("far",), ("c", 3), ("w", 0, 2), ("send",),
    ("w", 0, 3), ("w", 0, 4), ("reduce",), ("w", 0, 5), ("clip",), ("lows",),
]


def dot(a, b):
    return lax.dot_general(a, b, (((1,), (0,)), ((), ())), preferred_element_type=F32)


def dot_t(a, b):
    return lax.dot_general(a, b, (((0,), (0,)), ((), ())), preferred_element_type=F32)


class PlaneGather:
    def __init__(self, ref_of, rows, ssem, rsem, a, b, fs_of, direct=False):
        self.direct = direct
        self.ref_of, self.rows, self.ss, self.rs = ref_of, rows, ssem, rsem
        self.a, self.b, self.fs_of = a, b, fs_of
        self.am = [a, (a + 3) % SIDE, (a + 1) % SIDE, (a + 2) % SIDE]
        self.bp, self.bm, self.b2 = (b + 1) % SIDE, (b + 3) % SIDE, (b + 2) % SIDE
        self.sent = []

    def part(self, half):
        h = self.rows // 2
        return {None: (0, self.rows), 0: (0, h), 1: (h, h)}[half]

    def copy(self, j, block, half, to):
        lo, n = self.part(half)
        ref = self.ref_of(block, lo, n)
        return pltpu.make_async_remote_copy(
            src_ref=ref, dst_ref=ref, send_sem=self.ss.at[j], recv_sem=self.rs.at[j],
            device_id={FS: to}, device_id_type=pl.DeviceIdType.MESH)

    def send(self, j, block, half, to):
        c = self.copy(j, block, half, to)
        c.start()
        self.sent.append(c)

    def got(self, j, block, half):
        self.copy(j, block, half, block).wait_recv()

    def along_b(self, m):
        blk = self.fs_of(self.am[m], self.b)
        self.send(4 + 2 * m, blk, None, self.fs_of(self.a, self.bp))
        self.send(5 + 2 * m, blk, None, self.fs_of(self.a, self.bm))

    def start(self):
        own = self.fs_of(self.a, self.b)
        self.send(0, own, None, self.fs_of(self.am[2], self.b))
        self.send(1, own, None, self.fs_of(self.am[1], self.b))
        if self.direct:
            self.send(2, own, None, self.fs_of(self.am[3], self.b))
        self.along_b(0)
        return own

    def take_a(self, m):
        blk = self.fs_of(self.am[m], self.b)
        self.got(m - 1, blk, None)
        if not self.direct:
            self.send(m + 1, blk, m - 1, self.fs_of(self.am[3 - m], self.b))
        self.along_b(m)
        return blk

    def take_a2(self):
        blk = self.fs_of(self.am[3], self.b)
        if self.direct:
            self.got(2, blk, None)
        else:
            self.got(2, blk, 0)
            self.got(3, blk, 1)
        self.along_b(3)
        return blk

    def take_b(self, m):
        lo = self.fs_of(self.am[m], self.bm)
        self.got(4 + 2 * m, lo, None)
        self.send(12 + 2 * m, lo, 0, self.fs_of(self.a, self.bp))
        hi = self.fs_of(self.am[m], self.bp)
        self.got(5 + 2 * m, hi, None)
        self.send(13 + 2 * m, hi, 1, self.fs_of(self.a, self.bm))
        return lo, hi

    def take_b2(self, m):
        blk = self.fs_of(self.am[m], self.b2)
        self.got(12 + 2 * m, blk, 0)
        self.got(13 + 2 * m, blk, 1)
        return blk

    def finish(self):
        for c in self.sent:
            c.wait_send()


def moments(first, second, reduced, clip_scale):
    scaled = clip_scale * reduced
    first_new = beta_first * first + (1.0 - beta_first) * scaled
    second_new = beta_second * second + (1.0 - beta_second) * scaled * scaled
    return first_new, second_new, first_new / (jnp.sqrt(second_new) + epsilon)


def exchange_kernel(target, xq_h, gq_h, ho_h, go_h, pq_h, po_h, wq_h, wo_h, fq_h, sq_h, fo_h, so_h,
                    pf, pw, lowg, low, scale,
                    xq, gq, ho, go, wq, wo, fq, sq, fo, so, ho_t, gq_t, grad_o, grad_q, acc, acc_q, rs_out, rs_in,
                    sums,
                    in_sem, p_ss, p_rs, w_ss, w_rs, sib_ss, sib_rs, rs_ss, rs_rs,
                    sum_ss, sum_rs, ag_ss, ag_rs):
    i, t = lax.axis_index(FS), lax.axis_index(TP)
    z, y, c = i // SIDE, i % SIDE, t % 2
    a, b = y * (1 - c) + z * c, z * (1 - c) + y * c

    def fs_of(a_, b_):
        return a_ * (1 + 3 * c) + b_ * (4 - 3 * c)

    nq, no = pq_h.shape[0], po_h.shape[0]
    loads = []

    def load(src, dst):
        cp = pltpu.make_async_copy(src, dst, in_sem.at[len(loads)])
        cp.start()
        loads.append(cp)
        return cp

    half = (nq + no) // 2
    p1 = load(pq_h, pf.at[i, 0, pl.ds(0, nq)])
    p2 = load(po_h.at[pl.ds(0, half - nq)], pf.at[i, 0, pl.ds(nq, half - nq)])
    p3 = load(po_h.at[pl.ds(half - nq, half)], pf.at[i, 1])
    own_f32 = [load(s, d) for s, d in ((wq_h, wq), (wo_h, wo), (fq_h, fq), (fo_h, fo), (sq_h, sq), (so_h, so))]
    l_ho, l_gq = load(ho_h, ho), load(gq_h, gq)
    step = go.shape[1] // 4
    l_go = [load(go_h.at[:, pl.ds(k * step, step)], go.at[:, pl.ds(k * step, step)]) for k in range(4)]
    l_xq = load(xq_h, xq)

    barrier = pltpu.get_barrier_semaphore()
    nbrs = [{FS: fs_of((a + d) % SIDE, b)} for d in (1, 2, 3)] + [
        {FS: fs_of(a, (b + d) % SIDE)} for d in (1, 2, 3)]
    nbrs += [{TP: (t + d) % N_TP} for d in range(1, N_TP)]
    for n in nbrs:
        pl.semaphore_signal(barrier, inc=1, device_id=n, device_id_type=pl.DeviceIdType.MESH)
    for cp in (p1, p2, p3):
        cp.wait()
    pl.semaphore_wait(barrier, len(nbrs))

    piece = half // NP
    pgs = [PlaneGather(lambda blk, lo, n, g=g: pf.at[blk, c, pl.ds(g * piece + lo, n)], piece,
                       p_ss.at[g], p_rs.at[g], a, b, fs_of, direct=True) for g in range(NP)]
    wpiece = pw.shape[1] // NW
    wgs = [PlaneGather(lambda blk, lo, n, g=g: pw.at[blk, pl.ds(g * wpiece + lo, n)], wpiece,
                       w_ss.at[g], w_rs.at[g], a, b, fs_of) for g in range(NW)]
    sib = {TP: t + 1 - 2 * c}
    sib_sent = []

    def sib_copy(g, blk, which):
        ref = pf.at[blk, which, pl.ds(g * piece, piece)]
        return pltpu.make_async_remote_copy(
            src_ref=ref, dst_ref=ref, send_sem=sib_ss.at[g, blk], recv_sem=sib_rs.at[g, blk],
            device_id=sib, device_id_type=pl.DeviceIdType.MESH)

    def to_sib(g, *blks):
        for blk in blks:
            cp = sib_copy(g, blk, c)
            cp.start()
            sib_sent.append(cp)

    for g in pgs:
        g.start()

    for cp in own_f32:
        cp.wait()
    row = 0
    for src in (wq, wo, fq, fo, sq, so):
        for col in range(0, src.shape[1], 128):
            part = src[:, col:col + 128]
            if src is wq or src is wo:
                part = part * (1.0 - step_rate * decay_rate)
            pw[i, row:row + src.shape[0], :] = part.astype(BF16)
            row += src.shape[0]

    def w_stage(w, s):
        g = wgs[w]
        if s == 0:
            g.start()
        elif s == 1:
            g.take_a(1)
            g.take_a(2)
        elif s == 2:
            g.take_b(0)
            g.take_a2()
        elif s == 3:
            g.take_b(1)
            g.take_b(2)
        elif s == 4:
            g.take_b(3)
        else:
            for m in range(4):
                g.take_b2(m)

    def transposes():
        l_ho.wait()
        ho_t[...] = ho[...].T
        l_gq.wait()
        gq_t[...] = gq[...].T

    def gradient_o(k):
        if k % 4 == 0:
            l_go[k // 4].wait()
        grad_o[:, k * 256:k * 256 + 256] = dot(ho_t[...], go[:, k * 256:k * 256 + 256]).astype(BF16)

    def gradient_q(k):
        if k == 0:
            l_xq.wait()
        grad_q[:, k * 256:k * 256 + 256] = dot(gq_t[...], xq[:, k * 256:k * 256 + 256]).astype(BF16)

    def wait_sib(*blks):
        for blk in blks:
            for g in range(NP):
                sib_copy(g, blk, 1 - c).wait_recv()

    def project_o(*blks):
        out = None
        for blk in blks:
            p = pf[blk].reshape(2 * half, -1)[nq:]
            d = dot(grad_o[:, pl.ds(pl.multiple_of(blk * no, no), no)], p)
            out = d if out is None else out + d
        return out

    a1, a2, a3 = (a + 3) % SIDE, (a + 1) % SIDE, (a + 2) % SIDE
    b1, b2, b3 = (b + 3) % SIDE, (b + 1) % SIDE, (b + 2) % SIDE
    near = [fs_of(p, q) for p in (a1, a2) for q in (b1, b2)] + [fs_of(a, b1), fs_of(a, b2), fs_of(a1, b), fs_of(a2, b)]
    far = [fs_of(a3, b), fs_of(a, b3), fs_of(a3, b1), fs_of(a3, b2), fs_of(a1, b3), fs_of(a2, b3)]
    last = fs_of(a3, b3)

    def project_near():
        wait_sib(*near)
        acc[...] = project_o(i, *near)

    cq = fq.shape[1]

    def rs_copy(d):
        return pltpu.make_async_remote_copy(
            src_ref=rs_out.at[(i + d) % N_FS], dst_ref=rs_in.at[d], send_sem=rs_ss.at[d], recv_sem=rs_rs,
            device_id={FS: (i + d) % N_FS}, device_id_type=pl.DeviceIdType.MESH)

    def start(make):
        def body(d, _):
            make(d).start()
            return 0
        return body

    def wait_send(make):
        def body(d, _):
            make(d).wait_send()
            return 0
        return body

    def project_q(*zrows):
        out = None
        for zr in zrows:
            p = pf[pl.ds(zr * SIDE, SIDE), 0, 0:nq, :].reshape(SIDE * nq, -1)
            d = dot(grad_q[:, pl.ds(pl.multiple_of(zr * SIDE * nq, SIDE * nq), SIDE * nq)], p)
            out = d if out is None else out + d
        return out

    def project_far():
        wait_sib(*far)
        acc[...] += project_o(*far)
        acc_q[...] = project_q(z, (z + 1) % SIDE, (z + 3) % SIDE)

    def send_partials():
        wait_sib(last)
        part_o = acc[...] + project_o(last)
        part_q = acc_q[...] + project_q((z + 2) % SIDE)
        rs_out[:, :, cq:] = part_o.T.astype(BF16).reshape(N_FS, -1, part_o.shape[0])
        rs_out[:, :, :cq] = part_q.T.astype(BF16).reshape(N_FS, -1, part_q.shape[0])
        lax.fori_loop(1, N_FS, start(rs_copy), 0)

    me = i * N_TP + t

    def ag_copy(d):
        return pltpu.make_async_remote_copy(
            src_ref=lowg.at[i], dst_ref=lowg.at[i], send_sem=ag_ss.at[d], recv_sem=ag_rs.at[d],
            device_id={FS: (i + d) % N_FS}, device_id_type=pl.DeviceIdType.MESH)

    def arrivals(buf, me, n, axis, sems):
        def body(d, _):
            blk = (me - d + n) % n
            pltpu.make_async_remote_copy(
                src_ref=buf.at[blk], dst_ref=buf.at[blk], send_sem=sems.at[d], recv_sem=sems.at[d],
                device_id={axis: blk}, device_id_type=pl.DeviceIdType.MESH).wait_recv()
            return 0
        lax.fori_loop(1, n, body, 0)

    zs, ys, ts = [(z + d) % SIDE for d in range(SIDE)], [(y + d) % SIDE for d in range(SIDE)], []
    for d in range(N_TP):
        ts.append(((t // 2 + d // 2) % SIDE) * 2 + (c + d % 2) % 2)
    distance = lambda d: sum(min(k, SIDE - k) for k in (d[0], d[1], d[2] // 2)) * 2 + d[2] % 2
    far_first = sorted(((dz, dy, dt) for dz in range(SIDE) for dy in range(SIDE) for dt in range(N_TP)),
                       key=distance, reverse=True)[:-1]
    others = sums.at[pl.ds(0, N_FS * N_TP - 1)]

    def reduce_partials():
        arrived = rs_in.at[pl.ds(1, N_FS - 1)]
        pltpu.make_async_copy(arrived, arrived, rs_rs).wait()
        reduced = rs_out[i].astype(F32)
        for d in range(1, N_FS):
            reduced = reduced + rs_in[d].astype(F32)
        low[...] = reduced
        lowg[i] = reduced.astype(BF16)
        sums[me] = jnp.full(sums.shape[1:], jnp.sum(reduced * reduced), F32)
        for dz, dy, dt in far_first:
            pltpu.make_async_remote_copy(
                src_ref=sums.at[me], dst_ref=sums.at[me], send_sem=sum_ss, recv_sem=sum_rs,
                device_id={FS: zs[dz] * SIDE + ys[dy], TP: ts[dt]}, device_id_type=pl.DeviceIdType.MESH).start()
        lax.fori_loop(1, N_FS, start(ag_copy), 0)

    def clip():
        pltpu.make_async_copy(others, others, sum_rs).wait()
        scale[...] = jnp.broadcast_to(
            jnp.minimum(1.0, target / jnp.sqrt(jnp.sum(sums[...], axis=0))), scale.shape)

    def from_a(m):
        for g, pg in enumerate(pgs):
            to_sib(g, pg.take_a(m) if m < 3 else pg.take_a2())

    def from_b(m):
        for g, pg in enumerate(pgs):
            to_sib(g, *pg.take_b(m))

    def from_b2(m):
        for g, pg in enumerate(pgs):
            to_sib(g, pg.take_b2(m))

    steps = dict(a=from_a, b=from_b, c=from_b2, w=w_stage, t=transposes, g=gradient_o, q=gradient_q, near=project_near, far=project_far,
                 send=send_partials, reduce=reduce_partials, clip=clip,
                 lows=lambda: arrivals(lowg, i, N_FS, FS, ag_rs))
    for name, *args in ORDER:
        steps[name](*args)
    pltpu.make_async_copy(others, others, sum_ss).wait()
    for g in pgs + wgs:
        g.finish()
    for cp in sib_sent:
        cp.wait_send()
    lax.fori_loop(1, N_FS, wait_send(rs_copy), 0)
    lax.fori_loop(1, N_FS, wait_send(ag_copy), 0)


def update_kernel(pf, pw, lowg, low, scale, pq, po, wq, wo, fq, sq, fo, so,
                  nwq, nwo, nfq, nsq, nfo, nso, stq, sto, cpq, cpo, dirs):
    cq, co = fq.shape[1], fo.shape[1]
    nq, no, rows = pq.shape[0], po.shape[0], fq.shape[0]
    g = pl.program_id(0)
    n = cpq.shape[0] // nq
    blocks = (cq + co) // 128
    at_o = (cq // 128) * nq
    at_f = at_o + (co // 128) * no
    s = scale[0:1, 0:1]

    @pl.when(g == 0)
    def _():
        for j in range(blocks):
            f = pw[:, at_f + j * rows:at_f + (j + 1) * rows, :].astype(F32)
            v = pw[:, at_f + (blocks + j) * rows:at_f + (blocks + j + 1) * rows, :].astype(F32)
            l = lowg[:, :, j * 128:(j + 1) * 128].astype(F32)
            d = moments(f, v, l, s)[2]
            dirs[:, j * 128:(j + 1) * 128] = (-step_rate * d).reshape(-1, 128).astype(BF16)

    dq, do = dirs[:, :cq], dirs[:, cq:]
    own = pl.ds(g * n, n)
    whole = pf[own].reshape(n, nq + no, pf.shape[3])
    mq = dot(whole[:, :nq, :].reshape(n * nq, -1), dq)
    mo = dot(whole[:, nq:, :].reshape(n * no, -1), do)
    for col in range(0, cq, 128):
        w = pw[own, (col // 128) * nq:(col // 128 + 1) * nq, :].astype(F32).reshape(n * nq, 128)
        cpq[:, col:col + 128] = (w + mq[:, col:col + 128]).astype(BF16)
    for col in range(0, co, 128):
        at = at_o + (col // 128) * no
        w = pw[own, at:at + no, :].astype(F32).reshape(n * no, 128)
        cpo[:, col:col + 128] = (w + mo[:, col:col + 128]).astype(BF16)

    @pl.when(g == 0)
    def _():
        f, v, _ = moments(fq[...], sq[...], low[:, :cq], s)
        nfq[...] = f
        nsq[...] = v
        f, v, _ = moments(fo[...], so[...], low[:, cq:], s)
        nfo[...] = f
        nso[...] = v
        for p_, d_, w_, st_, nw_ in ((pq, dq, wq, stq, nwq), (po, do, wo, sto, nwo)):
            step = dot(p_[...], d_) * (-1.0 / step_rate) + decay_rate * w_[...]
            st_[...] = step
            nw_[...] = w_[...] - step_rate * step


def per_device(query_latent_rows, grad_q, head_out, grad_out, proj_q, proj_o, query_up_weight, weight_o,
               first_q, second_q, first_o, second_o):
    nq, no, rank = proj_q.shape[0], proj_o.shape[0], proj_q.shape[1]
    cq, co = first_q.shape[1], first_o.shape[1]
    rows = first_q.shape[0]
    target = math.sqrt(rows * N_FS * (cq + co) * N_TP)
    half = (nq + no) // 2
    wrows = (nq * cq + no * co + 2 * rows * (cq + co)) // 128
    sds = jax.ShapeDtypeStruct
    dma = pltpu.SemaphoreType.DMA
    V = pltpu.VMEM
    ins = (query_latent_rows, grad_q, head_out, grad_out, proj_q, proj_o, query_up_weight, weight_o,
           first_q, second_q, first_o, second_o)
    like = lambda x: V(x.shape, x.dtype)
    tokens = query_latent_rows.shape[0]

    def ex(*refs):
        exchange_kernel(target, *refs)

    gathered = pl.pallas_call(
        ex,
        out_shape=[V((N_FS, 2, half, rank), BF16), V((N_FS, wrows, 128), BF16),
                   V((N_FS, rows, cq + co), BF16), V((rows, cq + co), F32), V((8, 128), F32)],
        in_specs=[pl.BlockSpec(memory_space=pltpu.HBM)] * len(ins),
        out_specs=[pl.BlockSpec(memory_space=pltpu.VMEM)] * 5,
        scratch_shapes=[
            like(query_latent_rows), like(grad_q), like(head_out), like(grad_out),
            like(query_up_weight), like(weight_o), like(first_q), like(second_q), like(first_o), like(second_o),
            V((co, tokens), BF16), V((cq, tokens), BF16), V((co, N_FS * no), BF16), V((cq, N_FS * nq), BF16),
            V((co, rank), F32), V((cq, rank), F32), V((N_FS, rows, cq + co), BF16), V((N_FS, rows, cq + co), BF16),
            V((N_FS * N_TP, 1, 128), F32),
            dma((16,)), dma((NP, 20)), dma((NP, 20)), dma((NW, 20)), dma((NW, 20)),
            dma((NP, N_FS)), dma((NP, N_FS)),
            dma((N_FS,)), dma, dma, dma, dma((N_FS,)), dma((N_FS,)),
        ],
        compiler_params=pltpu.CompilerParams(collective_id=0, has_side_effects=True,
                                             vmem_limit_bytes=48 * 1024 * 1024),
        name="exchange",
    )(*[pltpu.with_memory_space_constraint(x, pltpu.HBM) for x in ins])

    G = 2
    n = N_FS // G
    full = lambda x: pl.BlockSpec(x.shape, lambda g: (0,) * len(x.shape))
    outs = [sds((nq, cq), F32), sds((no, co), F32), sds((rows, cq), F32), sds((rows, cq), F32),
            sds((rows, co), F32), sds((rows, co), F32), sds((nq, cq), F32), sds((no, co), F32)]
    ops = (*gathered, proj_q, proj_o, query_up_weight, weight_o, first_q, second_q, first_o, second_o)
    return tuple(pl.pallas_call(
        update_kernel,
        grid=(G,),
        in_specs=[full(x) for x in ops],
        out_specs=[full(o) for o in outs] + [pl.BlockSpec((n * nq, cq), lambda g: (g, 0)),
                                             pl.BlockSpec((n * no, co), lambda g: (g, 0))],
        out_shape=outs + [sds((N_FS * nq, cq), BF16), sds((N_FS * no, co), BF16)],
        scratch_shapes=[V((rows * N_FS, cq + co), BF16)],
        compiler_params=pltpu.CompilerParams(vmem_limit_bytes=24 * 1024 * 1024),
        name="update",
    )(*ops))


def solution(mesh):
    rows, both, cols = P(FS, None), P(FS, TP), P(None, TP)
    return jax.shard_map(
        per_device,
        mesh=mesh,
        in_specs=(rows, both, both, rows, rows, rows) + (both,) * 6,
        out_specs=(both,) * 8 + (cols, cols),
        check_vma=False,
    )
```

```python
import math

import jax
import jax.numpy as jnp
from jax import lax
from jax.experimental import pallas as pl
from jax.experimental.pallas import tpu as pltpu
from jax.sharding import PartitionSpec as P

FS, TP = "fs", "tp"
SIDE = 4
N_FS, N_TP = 16, 8

beta_first = 0.8
beta_second = 0.9
epsilon = 1e-08
decay_rate = 2.0
step_rate = 0.05

BF16, F32 = jnp.bfloat16, jnp.float32

CHUNKS = 4
NW = 1
ORDER = [('w', 0, 0), ('t',), ('g', 0), ('g', 1), ('g', 2), ('a', 1), ('a', 2), ('b', 0), ('g', 3), ('a', 3), ('g', 4), ('g', 5), ('xa', 1), ('xa', 2), ('xb', 0), ('b', 1), ('b', 2), ('g', 6), ('g', 7), ('b', 3), ('w', 0, 1), ('xa', 3), ('c', 0), ('g', 8), ('g', 9), ('xb', 1), ('xb', 2), ('c', 1), ('c', 2), ('g', 10), ('g', 11), ('xb', 3), ('c', 3), ('xc', 0), ('w', 0, 2), ('g', 12), ('g', 13), ('g', 14), ('g', 15), ('q', 0), ('q', 1), ('xc', 1), ('xc', 2), ('q', 2), ('q', 3), ('xc', 3), ('near',), ('far',), ('w', 0, 3), ('send',), ('w', 0, 4), ('reduce',), ('w', 0, 5), ('clip',), ('lows',)]


def dot(a, b):
    return lax.dot_general(a, b, (((1,), (0,)), ((), ())), preferred_element_type=F32)


def dot_t(a, b):
    return lax.dot_general(a, b, (((0,), (0,)), ((), ())), preferred_element_type=F32)


class PlaneGather:
    def __init__(self, ref_of, rows, ssem, rsem, a, b, fs_of, direct=False):
        self.direct = direct
        self.ref_of, self.rows, self.ss, self.rs = ref_of, rows, ssem, rsem
        self.a, self.b, self.fs_of = a, b, fs_of
        self.am = [a, (a + 3) % SIDE, (a + 1) % SIDE, (a + 2) % SIDE]
        self.bp, self.bm, self.b2 = (b + 1) % SIDE, (b + 3) % SIDE, (b + 2) % SIDE
        self.sent = []

    def part(self, half):
        h = self.rows // 2
        return {None: (0, self.rows), 0: (0, h), 1: (h, h)}[half]

    def copy(self, j, block, half, to):
        lo, n = self.part(half)
        ref = self.ref_of(block, lo, n)
        return pltpu.make_async_remote_copy(
            src_ref=ref, dst_ref=ref, send_sem=self.ss.at[j], recv_sem=self.rs.at[j],
            device_id={FS: to}, device_id_type=pl.DeviceIdType.MESH)

    def send(self, j, block, half, to):
        c = self.copy(j, block, half, to)
        c.start()
        self.sent.append(c)

    def got(self, j, block, half):
        self.copy(j, block, half, block).wait_recv()

    def along_b(self, m):
        blk = self.fs_of(self.am[m], self.b)
        self.send(4 + 2 * m, blk, None, self.fs_of(self.a, self.bp))
        self.send(5 + 2 * m, blk, None, self.fs_of(self.a, self.bm))

    def start(self):
        own = self.fs_of(self.a, self.b)
        self.send(0, own, None, self.fs_of(self.am[2], self.b))
        self.send(1, own, None, self.fs_of(self.am[1], self.b))
        if self.direct:
            self.send(2, own, None, self.fs_of(self.am[3], self.b))
        self.along_b(0)
        return own

    def take_a(self, m):
        blk = self.fs_of(self.am[m], self.b)
        self.got(m - 1, blk, None)
        if not self.direct:
            self.send(m + 1, blk, m - 1, self.fs_of(self.am[3 - m], self.b))
        self.along_b(m)
        return blk

    def take_a2(self):
        blk = self.fs_of(self.am[3], self.b)
        if self.direct:
            self.got(2, blk, None)
        else:
            self.got(2, blk, 0)
            self.got(3, blk, 1)
        self.along_b(3)
        return blk

    def take_b(self, m):
        lo = self.fs_of(self.am[m], self.bm)
        self.got(4 + 2 * m, lo, None)
        self.send(12 + 2 * m, lo, 0, self.fs_of(self.a, self.bp))
        hi = self.fs_of(self.am[m], self.bp)
        self.got(5 + 2 * m, hi, None)
        self.send(13 + 2 * m, hi, 1, self.fs_of(self.a, self.bm))
        return lo, hi

    def take_b2(self, m):
        blk = self.fs_of(self.am[m], self.b2)
        self.got(12 + 2 * m, blk, 0)
        self.got(13 + 2 * m, blk, 1)
        return blk

    def finish(self):
        for c in self.sent:
            c.wait_send()


def moments(first, second, reduced, clip_scale):
    scaled = clip_scale * reduced
    first_new = beta_first * first + (1.0 - beta_first) * scaled
    second_new = beta_second * second + (1.0 - beta_second) * scaled * scaled
    return first_new, second_new, first_new / (jnp.sqrt(second_new) + epsilon)


def exchange_kernel(target, xq_h, gq_h, ho_h, go_h, pq_h, po_h, wq_h, wo_h, fq_h, sq_h, fo_h, so_h,
                    pf, pw, lowg, low, scale,
                    xq, gq, ho, go, wq, wo, fq, sq, fo, so, ho_t, gq_t, grad_o, grad_q, acc, acc_q, rs_out, rs_in,
                    sums,
                    in_sem, p_ss, p_rs, w_ss, w_rs, sib_ss, sib_rs, x_ss, x_rs, rs_ss, rs_rs,
                    sum_ss, sum_rs, ag_ss, ag_rs):
    i, t = lax.axis_index(FS), lax.axis_index(TP)
    z, y, c = i // SIDE, i % SIDE, t % 2
    a, b = y * (1 - c) + z * c, z * (1 - c) + y * c

    def fs_of(a_, b_):
        return a_ * (1 + 3 * c) + b_ * (4 - 3 * c)

    nq, no = pq_h.shape[0], po_h.shape[0]
    loads = []

    def load(src, dst):
        cp = pltpu.make_async_copy(src, dst, in_sem.at[len(loads)])
        cp.start()
        loads.append(cp)
        return cp

    half = (nq + no) // 2
    p1 = load(pq_h, pf.at[i, 0, pl.ds(0, nq)])
    p2 = load(po_h.at[pl.ds(0, half - nq)], pf.at[i, 0, pl.ds(nq, half - nq)])
    p3 = load(po_h.at[pl.ds(half - nq, half)], pf.at[i, 1])
    own_f32 = [load(s, d) for s, d in ((wq_h, wq), (wo_h, wo), (fq_h, fq), (fo_h, fo), (sq_h, sq), (so_h, so))]
    l_ho, l_gq = load(ho_h, ho), load(gq_h, gq)
    step = go.shape[1] // 4
    l_go = [load(go_h.at[:, pl.ds(k * step, step)], go.at[:, pl.ds(k * step, step)]) for k in range(4)]
    l_xq = load(xq_h, xq)

    barrier = pltpu.get_barrier_semaphore()
    nbrs = [{FS: fs_of((a + d) % SIDE, b)} for d in (1, 2, 3)] + [
        {FS: fs_of(a, (b + d) % SIDE)} for d in (1, 2, 3)]
    nbrs += [{TP: (t + d) % N_TP} for d in range(1, N_TP)]
    for n in nbrs:
        pl.semaphore_signal(barrier, inc=1, device_id=n, device_id_type=pl.DeviceIdType.MESH)
    for cp in (p1, p2, p3):
        cp.wait()
    pl.semaphore_wait(barrier, len(nbrs))

    quarter = half // 2
    par = (t // 2) % 2
    pg = PlaneGather(lambda blk, lo, n: pf.at[blk, c, pl.ds(pl.multiple_of(par * quarter, 16) + lo, n)], quarter,
                     p_ss, p_rs, a, b, fs_of, direct=True)
    wpiece = pw.shape[1] // NW
    wgs = [PlaneGather(lambda blk, lo, n, g=g: pw.at[blk, pl.ds(g * wpiece + lo, n)], wpiece,
                       w_ss.at[g], w_rs.at[g], a, b, fs_of) for g in range(NW)]
    sib = {TP: t + 1 - 2 * c}
    sent = []

    def sib_copy(blk, which):
        ref = pf.at[blk, which]
        return pltpu.make_async_remote_copy(
            src_ref=ref, dst_ref=ref, send_sem=sib_ss.at[blk], recv_sem=sib_rs.at[blk],
            device_id=sib, device_id_type=pl.DeviceIdType.MESH)

    def x_copy(blk, parity, side):
        ref = pf.at[blk, c, pl.ds(pl.multiple_of(parity * quarter, 16) + side * (quarter // 2), quarter // 2)]
        return pltpu.make_async_remote_copy(
            src_ref=ref, dst_ref=ref, send_sem=x_ss.at[side, blk], recv_sem=x_rs.at[side, blk],
            device_id={TP: ((t // 2 + (1, 3)[side]) % SIDE) * 2 + c}, device_id_type=pl.DeviceIdType.MESH)

    def to_x(*blks):
        for blk in blks:
            for side in (0, 1):
                cp = x_copy(blk, par, side)
                cp.start()
                sent.append(cp)

    def from_x(*blks):
        for blk in blks:
            for side in (0, 1):
                x_copy(blk, 1 - par, side).wait_recv()
            cp = sib_copy(blk, c)
            cp.start()
            sent.append(cp)

    pg.start()

    for cp in own_f32:
        cp.wait()
    row = 0
    for src in (wq, wo, fq, fo, sq, so):
        for col in range(0, src.shape[1], 128):
            part = src[:, col:col + 128]
            if src is wq or src is wo:
                part = part * (1.0 - step_rate * decay_rate)
            pw[i, row:row + src.shape[0], :] = part.astype(BF16)
            row += src.shape[0]

    def w_stage(w, s):
        g = wgs[w]
        if s == 0:
            g.start()
        elif s == 1:
            g.take_a(1)
            g.take_a(2)
        elif s == 2:
            g.take_b(0)
            g.take_a2()
        elif s == 3:
            g.take_b(1)
            g.take_b(2)
        elif s == 4:
            g.take_b(3)
        else:
            for m in range(4):
                g.take_b2(m)

    def transposes():
        l_ho.wait()
        ho_t[...] = ho[...].T
        l_gq.wait()
        gq_t[...] = gq[...].T

    def gradient_o(k):
        if k % 4 == 0:
            l_go[k // 4].wait()
        grad_o[:, k * 256:k * 256 + 256] = dot(ho_t[...], go[:, k * 256:k * 256 + 256]).astype(BF16)

    def gradient_q(k):
        if k == 0:
            l_xq.wait()
        grad_q[:, k * 256:k * 256 + 256] = dot(gq_t[...], xq[:, k * 256:k * 256 + 256]).astype(BF16)

    def wait_sib(*blks):
        for blk in blks:
            sib_copy(blk, 1 - c).wait_recv()

    def project_o(*blks):
        out = None
        for blk in blks:
            p = pf[blk].reshape(2 * half, -1)[nq:]
            d = dot(grad_o[:, pl.ds(pl.multiple_of(blk * no, no), no)], p)
            out = d if out is None else out + d
        return out

    a1, a2, a3 = (a + 3) % SIDE, (a + 1) % SIDE, (a + 2) % SIDE
    b1, b2, b3 = (b + 3) % SIDE, (b + 1) % SIDE, (b + 2) % SIDE
    near = [fs_of(p, q) for p in (a1, a2) for q in (b1, b2)] + [fs_of(a, b1), fs_of(a, b2), fs_of(a1, b), fs_of(a2, b)]
    far = [fs_of(a3, b), fs_of(a, b3), fs_of(a3, b1), fs_of(a3, b2), fs_of(a1, b3), fs_of(a2, b3)]
    last = fs_of(a3, b3)

    def project_near():
        wait_sib(*near)
        acc[...] = project_o(i, *near)

    cq = fq.shape[1]

    zs, ys, ts = [(z + d) % SIDE for d in range(SIDE)], [(y + d) % SIDE for d in range(SIDE)], []
    for d in range(N_TP):
        ts.append(((t // 2 + d // 2) % SIDE) * 2 + (c + d % 2) % 2)
    distance = lambda d: sum(min(k, SIDE - k) for k in (d[0], d[1], d[2] // 2)) * 2 + d[2] % 2
    far_first = sorted(((dz, dy, dt) for dz in range(SIDE) for dy in range(SIDE) for dt in range(N_TP)),
                       key=distance, reverse=True)[:-1]
    plane_far_first = [(dz, dy) for dz, dy, dt in far_first if dt == 0]

    def rs_copy(dz, dy):
        d, to = dz * SIDE + dy, zs[dz] * SIDE + ys[dy]
        return pltpu.make_async_remote_copy(
            src_ref=rs_out.at[to], dst_ref=rs_in.at[d], send_sem=rs_ss.at[d], recv_sem=rs_rs,
            device_id={FS: to}, device_id_type=pl.DeviceIdType.MESH)

    def project_q(*zrows):
        out = None
        for zr in zrows:
            p = pf[pl.ds(zr * SIDE, SIDE), 0, 0:nq, :].reshape(SIDE * nq, -1)
            d = dot(grad_q[:, pl.ds(pl.multiple_of(zr * SIDE * nq, SIDE * nq), SIDE * nq)], p)
            out = d if out is None else out + d
        return out

    def project_far():
        wait_sib(*far)
        acc[...] += project_o(*far)
        acc_q[...] = project_q(z, (z + 1) % SIDE, (z + 3) % SIDE)

    def send_partials():
        wait_sib(last)
        part_o = acc[...] + project_o(last)
        part_q = acc_q[...] + project_q((z + 2) % SIDE)
        rs_out[:, :, cq:] = part_o.T.astype(BF16).reshape(N_FS, -1, part_o.shape[0])
        rs_out[:, :, :cq] = part_q.T.astype(BF16).reshape(N_FS, -1, part_q.shape[0])
        for dz, dy in plane_far_first:
            rs_copy(dz, dy).start()

    me = i * N_TP + t

    def ag_copy(dz, dy, back=False):
        d, to = dz * SIDE + dy, zs[dz] * SIDE + ys[dy]
        ref = lowg.at[zs[-dz] * SIDE + ys[-dy] if back else i]
        return pltpu.make_async_remote_copy(
            src_ref=ref, dst_ref=ref, send_sem=ag_ss.at[d], recv_sem=ag_rs.at[d],
            device_id={FS: to}, device_id_type=pl.DeviceIdType.MESH)

    def lows():
        for dz, dy in plane_far_first:
            ag_copy(dz, dy, back=True).wait_recv()

    others = sums.at[pl.ds(0, N_FS * N_TP - 1)]

    def reduce_partials():
        arrived = rs_in.at[pl.ds(1, N_FS - 1)]
        pltpu.make_async_copy(arrived, arrived, rs_rs).wait()
        reduced = rs_out[i].astype(F32)
        for d in range(1, N_FS):
            reduced = reduced + rs_in[d].astype(F32)
        low[...] = reduced
        lowg[i] = reduced.astype(BF16)
        sums[me] = jnp.full(sums.shape[1:], jnp.sum(reduced * reduced), F32)
        for dz, dy, dt in far_first:
            pltpu.make_async_remote_copy(
                src_ref=sums.at[me], dst_ref=sums.at[me], send_sem=sum_ss, recv_sem=sum_rs,
                device_id={FS: zs[dz] * SIDE + ys[dy], TP: ts[dt]}, device_id_type=pl.DeviceIdType.MESH).start()
        for dz, dy in plane_far_first:
            ag_copy(dz, dy).start()

    def clip():
        pltpu.make_async_copy(others, others, sum_rs).wait()
        scale[...] = jnp.broadcast_to(
            jnp.minimum(1.0, target / jnp.sqrt(jnp.sum(sums[...], axis=0))), scale.shape)

    along_a = [a, a1, a2, a3]
    steps = dict(a=lambda m: to_x(pg.take_a(m) if m < 3 else pg.take_a2()), b=lambda m: to_x(*pg.take_b(m)),
                 c=lambda m: to_x(pg.take_b2(m)), xa=lambda m: from_x(fs_of(along_a[m], b)),
                 xb=lambda m: from_x(fs_of(along_a[m], b1), fs_of(along_a[m], b2)),
                 xc=lambda m: from_x(fs_of(along_a[m], b3)), w=w_stage, t=transposes, g=gradient_o, q=gradient_q, near=project_near, far=project_far,
                 send=send_partials, reduce=reduce_partials, clip=clip,
                 lows=lows)
    for name, *args in ORDER:
        steps[name](*args)
    pltpu.make_async_copy(others, others, sum_ss).wait()
    for g in [pg] + wgs:
        g.finish()
    for cp in sent:
        cp.wait_send()
    for dz, dy in plane_far_first:
        rs_copy(dz, dy).wait_send()
    for dz, dy in plane_far_first:
        ag_copy(dz, dy).wait_send()


def update_kernel(pf, pw, lowg, low, scale, pq, po, wq, wo, fq, sq, fo, so, *refs):
    held, (dirs, *bufs, sems) = refs[:10], refs[10:]
    nwq, nwo, nfq, nsq, nfo, nso, stq, sto, cpq, cpo = bufs
    cq, co = fq.shape[1], fo.shape[1]
    nq, no, rows = pq.shape[0], po.shape[0], fq.shape[0]
    n = N_FS // CHUNKS
    blocks = (cq + co) // 128
    at_o = (cq // 128) * nq
    at_f = at_o + (co // 128) * no
    s = scale[0:1, 0:1]
    outgoing = []

    def write(k, part=None):
        src, dst = bufs[k], held[k]
        if part is not None:
            src, dst = src.at[part], dst.at[part]
        cp = pltpu.make_async_copy(src, dst, sems.at[len(outgoing)])
        cp.start()
        outgoing.append(cp)

    for j in range(blocks):
        f = pw[:, at_f + j * rows:at_f + (j + 1) * rows, :].astype(F32)
        v = pw[:, at_f + (blocks + j) * rows:at_f + (blocks + j + 1) * rows, :].astype(F32)
        l = lowg[:, :, j * 128:(j + 1) * 128].astype(F32)
        d = moments(f, v, l, s)[2]
        dirs[:, j * 128:(j + 1) * 128] = (-step_rate * d).reshape(-1, 128).astype(BF16)
    dq, do = dirs[:, :cq], dirs[:, cq:]

    for g in range(CHUNKS):
        own = slice(g * n, (g + 1) * n)
        whole = pf[own].reshape(n, nq + no, pf.shape[3])
        mo = dot(whole[:, nq:, :].reshape(n * no, -1), do)
        at = pl.ds(g * n * no, n * no)
        for col in range(0, co, 128):
            lo = at_o + (col // 128) * no
            w = pw[own, lo:lo + no, :].astype(F32).reshape(n * no, 128)
            cpo[at, col:col + 128] = (w + mo[:, col:col + 128]).astype(BF16)
        write(9, at)
        mq = dot(whole[:, :nq, :].reshape(n * nq, -1), dq)
        at = pl.ds(g * n * nq, n * nq)
        for col in range(0, cq, 128):
            w = pw[own, (col // 128) * nq:(col // 128 + 1) * nq, :].astype(F32).reshape(n * nq, 128)
            cpq[at, col:col + 128] = (w + mq[:, col:col + 128]).astype(BF16)
        write(8, at)
        if g == 0:
            for p_, d_, w_, st_, nw_ in ((pq, dq, wq, stq, nwq), (po, do, wo, sto, nwo)):
                step = dot(p_[...], d_) * (-1.0 / step_rate) + decay_rate * w_[...]
                st_[...] = step
                nw_[...] = w_[...] - step_rate * step
            for k in (6, 7, 0, 1):
                write(k)
            nfq[...], nsq[...], _ = moments(fq[...], sq[...], low[:, :cq], s)
            nfo[...], nso[...], _ = moments(fo[...], so[...], low[:, cq:], s)
            for k in (2, 3, 4, 5):
                write(k)
    for cp in outgoing:
        cp.wait()


def per_device(query_latent_rows, grad_q, head_out, grad_out, proj_q, proj_o, query_up_weight, weight_o,
               first_q, second_q, first_o, second_o):
    nq, no, rank = proj_q.shape[0], proj_o.shape[0], proj_q.shape[1]
    cq, co = first_q.shape[1], first_o.shape[1]
    rows = first_q.shape[0]
    target = math.sqrt(rows * N_FS * (cq + co) * N_TP)
    half = (nq + no) // 2
    wrows = (nq * cq + no * co + 2 * rows * (cq + co)) // 128
    sds = jax.ShapeDtypeStruct
    dma = pltpu.SemaphoreType.DMA
    V = pltpu.VMEM
    ins = (query_latent_rows, grad_q, head_out, grad_out, proj_q, proj_o, query_up_weight, weight_o,
           first_q, second_q, first_o, second_o)
    like = lambda x: V(x.shape, x.dtype)
    tokens = query_latent_rows.shape[0]

    def ex(*refs):
        exchange_kernel(target, *refs)

    gathered = pl.pallas_call(
        ex,
        out_shape=[V((N_FS, 2, half, rank), BF16), V((N_FS, wrows, 128), BF16),
                   V((N_FS, rows, cq + co), BF16), V((rows, cq + co), F32), V((8, 128), F32)],
        in_specs=[pl.BlockSpec(memory_space=pltpu.HBM)] * len(ins),
        out_specs=[pl.BlockSpec(memory_space=pltpu.VMEM)] * 5,
        scratch_shapes=[
            like(query_latent_rows), like(grad_q), like(head_out), like(grad_out),
            like(query_up_weight), like(weight_o), like(first_q), like(second_q), like(first_o), like(second_o),
            V((co, tokens), BF16), V((cq, tokens), BF16), V((co, N_FS * no), BF16), V((cq, N_FS * nq), BF16),
            V((co, rank), F32), V((cq, rank), F32), V((N_FS, rows, cq + co), BF16), V((N_FS, rows, cq + co), BF16),
            V((N_FS * N_TP, 1, 128), F32),
            dma((16,)), dma((20,)), dma((20,)), dma((NW, 20)), dma((NW, 20)),
            dma((N_FS,)), dma((N_FS,)), dma((2, N_FS)), dma((2, N_FS)),
            dma((N_FS,)), dma, dma, dma, dma((N_FS,)), dma((N_FS,)),
        ],
        compiler_params=pltpu.CompilerParams(collective_id=0, has_side_effects=True,
                                             vmem_limit_bytes=48 * 1024 * 1024),
        name="exchange",
    )(*[pltpu.with_memory_space_constraint(x, pltpu.HBM) for x in ins])

    outs = [sds((nq, cq), F32), sds((no, co), F32), sds((rows, cq), F32), sds((rows, cq), F32),
            sds((rows, co), F32), sds((rows, co), F32), sds((nq, cq), F32), sds((no, co), F32),
            sds((N_FS * nq, cq), BF16), sds((N_FS * no, co), BF16)]
    ops = (*gathered, proj_q, proj_o, query_up_weight, weight_o, first_q, second_q, first_o, second_o)
    return tuple(pl.pallas_call(
        update_kernel,
        in_specs=[pl.BlockSpec(memory_space=pltpu.VMEM)] * len(ops),
        out_specs=[pl.BlockSpec(memory_space=pltpu.HBM)] * len(outs),
        out_shape=outs,
        scratch_shapes=[V((rows * N_FS, cq + co), BF16)] + [like(o) for o in outs] + [dma((8 + 2 * CHUNKS,))],
        compiler_params=pltpu.CompilerParams(vmem_limit_bytes=24 * 1024 * 1024),
        name="update",
    )(*ops))


def solution(mesh):
    rows, both, cols = P(FS, None), P(FS, TP), P(None, TP)
    return jax.shard_map(
        per_device,
        mesh=mesh,
        in_specs=(rows, both, both, rows, rows, rows) + (both,) * 6,
        out_specs=(both,) * 8 + (cols, cols),
        check_vma=False,
    )
```

```python
import math

import jax
import jax.numpy as jnp
from jax import lax
from jax.experimental import pallas as pl
from jax.experimental.pallas import tpu as pltpu
from jax.sharding import PartitionSpec as P

FS, TP = "fs", "tp"
SIDE = 4
N_FS, N_TP = 16, 8

beta_first = 0.8
beta_second = 0.9
epsilon = 1e-08
decay_rate = 2.0
step_rate = 0.05

BF16, F32 = jnp.bfloat16, jnp.float32

CHUNKS = 4
NW = 1
ORDER = [
    ("w", 0, 0), ("t",), ("g", 0), ("g", 1), ("g", 2), ("a", 1), ("a", 2),
    ("b", 0), ("g", 3), ("a", 3), ("g", 4), ("g", 5), ("xa", 1), ("xa", 2),
    ("xb", 0), ("b", 1), ("b", 2), ("g", 6), ("g", 7), ("b", 3), ("w", 0, 1),
    ("xa", 3), ("c", 0), ("g", 8), ("g", 9), ("xb", 1), ("xb", 2), ("c", 1),
    ("c", 2), ("g", 10), ("g", 11), ("xb", 3), ("c", 3), ("w", 0, 2), ("xc", 0),
    ("g", 12), ("g", 13), ("g", 14), ("g", 15), ("q", 0), ("q", 1), ("xc", 1),
    ("xc", 2), ("q", 2), ("q", 3), ("xc", 3), ("near",), ("far",), ("send",),
    ("w", 0, 3), ("w", 0, 4), ("reduce",), ("clip",), ("w", 0, 5), ("lows",),
]


def dot(a, b):
    return lax.dot_general(a, b, (((1,), (0,)), ((), ())), preferred_element_type=F32)


def dot_t(a, b):
    return lax.dot_general(a, b, (((0,), (0,)), ((), ())), preferred_element_type=F32)


class PlaneGather:
    def __init__(self, ref_of, rows, ssem, rsem, a, b, fs_of, direct=False):
        self.direct = direct
        self.ref_of, self.rows, self.ss, self.rs = ref_of, rows, ssem, rsem
        self.a, self.b, self.fs_of = a, b, fs_of
        self.am = [a, (a + 3) % SIDE, (a + 1) % SIDE, (a + 2) % SIDE]
        self.bp, self.bm, self.b2 = (b + 1) % SIDE, (b + 3) % SIDE, (b + 2) % SIDE
        self.sent = []

    def part(self, half):
        h = self.rows // 2
        return {None: (0, self.rows), 0: (0, h), 1: (h, h)}[half]

    def copy(self, j, block, half, to):
        lo, n = self.part(half)
        ref = self.ref_of(block, lo, n)
        return pltpu.make_async_remote_copy(
            src_ref=ref, dst_ref=ref, send_sem=self.ss.at[j], recv_sem=self.rs.at[j],
            device_id={FS: to}, device_id_type=pl.DeviceIdType.MESH)

    def send(self, j, block, half, to):
        c = self.copy(j, block, half, to)
        c.start()
        self.sent.append(c)

    def got(self, j, block, half):
        self.copy(j, block, half, block).wait_recv()

    def along_b(self, m):
        blk = self.fs_of(self.am[m], self.b)
        self.send(4 + 2 * m, blk, None, self.fs_of(self.a, self.bp))
        self.send(5 + 2 * m, blk, None, self.fs_of(self.a, self.bm))

    def start(self):
        own = self.fs_of(self.a, self.b)
        self.send(0, own, None, self.fs_of(self.am[2], self.b))
        self.send(1, own, None, self.fs_of(self.am[1], self.b))
        if self.direct:
            self.send(2, own, None, self.fs_of(self.am[3], self.b))
        self.along_b(0)
        return own

    def take_a(self, m):
        blk = self.fs_of(self.am[m], self.b)
        self.got(m - 1, blk, None)
        if not self.direct:
            self.send(m + 1, blk, m - 1, self.fs_of(self.am[3 - m], self.b))
        self.along_b(m)
        return blk

    def take_a2(self):
        blk = self.fs_of(self.am[3], self.b)
        if self.direct:
            self.got(2, blk, None)
        else:
            self.got(2, blk, 0)
            self.got(3, blk, 1)
        self.along_b(3)
        return blk

    def take_b(self, m):
        lo = self.fs_of(self.am[m], self.bm)
        self.got(4 + 2 * m, lo, None)
        self.send(12 + 2 * m, lo, 0, self.fs_of(self.a, self.bp))
        hi = self.fs_of(self.am[m], self.bp)
        self.got(5 + 2 * m, hi, None)
        self.send(13 + 2 * m, hi, 1, self.fs_of(self.a, self.bm))
        return lo, hi

    def take_b2(self, m):
        blk = self.fs_of(self.am[m], self.b2)
        self.got(12 + 2 * m, blk, 0)
        self.got(13 + 2 * m, blk, 1)
        return blk

    def finish(self):
        for c in self.sent:
            c.wait_send()


def moments(first, second, reduced, clip_scale):
    scaled = clip_scale * reduced
    first_new = beta_first * first + (1.0 - beta_first) * scaled
    second_new = beta_second * second + (1.0 - beta_second) * scaled * scaled
    return first_new, second_new, first_new / (jnp.sqrt(second_new) + epsilon)


def exchange_kernel(target, xq_h, gq_h, ho_h, go_h, pq_h, po_h, wq_h, wo_h, fq_h, sq_h, fo_h, so_h,
                    pf, pw, lowg, low, scale,
                    xq, gq, ho, go, wq, wo, fq, sq, fo, so, ho_t, gq_t, grad_o, grad_q, acc, acc_q, rs_out, rs_in,
                    sums,
                    in_sem, p_ss, p_rs, w_ss, w_rs, sib_ss, sib_rs, x_ss, x_rs, rs_ss, rs_rs,
                    sum_ss, sum_rs, ag_ss, ag_rs):
    i, t = lax.axis_index(FS), lax.axis_index(TP)
    z, y, c = i // SIDE, i % SIDE, t % 2
    a, b = y * (1 - c) + z * c, z * (1 - c) + y * c

    def fs_of(a_, b_):
        return a_ * (1 + 3 * c) + b_ * (4 - 3 * c)

    nq, no = pq_h.shape[0], po_h.shape[0]
    loads = []

    def load(src, dst):
        cp = pltpu.make_async_copy(src, dst, in_sem.at[len(loads)])
        cp.start()
        loads.append(cp)
        return cp

    half = (nq + no) // 2
    p1 = load(pq_h, pf.at[i, 0, pl.ds(0, nq)])
    p2 = load(po_h.at[pl.ds(0, half - nq)], pf.at[i, 0, pl.ds(nq, half - nq)])
    p3 = load(po_h.at[pl.ds(half - nq, half)], pf.at[i, 1])
    own_f32 = [load(s, d) for s, d in ((wq_h, wq), (wo_h, wo), (fq_h, fq), (fo_h, fo), (sq_h, sq), (so_h, so))]
    l_ho, l_gq = load(ho_h, ho), load(gq_h, gq)
    step = go.shape[1] // 4
    l_go = [load(go_h.at[:, pl.ds(k * step, step)], go.at[:, pl.ds(k * step, step)]) for k in range(4)]
    l_xq = load(xq_h, xq)

    barrier = pltpu.get_barrier_semaphore()
    nbrs = [{FS: fs_of((a + d) % SIDE, b)} for d in (1, 2, 3)] + [
        {FS: fs_of(a, (b + d) % SIDE)} for d in (1, 2, 3)]
    nbrs += [{TP: (t + d) % N_TP} for d in range(1, N_TP)]
    for n in nbrs:
        pl.semaphore_signal(barrier, inc=1, device_id=n, device_id_type=pl.DeviceIdType.MESH)
    for cp in (p1, p2, p3):
        cp.wait()
    pl.semaphore_wait(barrier, len(nbrs))

    quarter = half // 2
    par = (t // 2) % 2
    pg = PlaneGather(lambda blk, lo, n: pf.at[blk, c, pl.ds(pl.multiple_of(par * quarter, 16) + lo, n)], quarter,
                     p_ss, p_rs, a, b, fs_of, direct=True)
    wpiece = pw.shape[1] // NW
    wgs = [PlaneGather(lambda blk, lo, n, g=g: pw.at[blk, pl.ds(g * wpiece + lo, n)], wpiece,
                       w_ss.at[g], w_rs.at[g], a, b, fs_of) for g in range(NW)]
    sib = {TP: t + 1 - 2 * c}
    sent = []

    def sib_copy(blk, which):
        ref = pf.at[blk, which]
        return pltpu.make_async_remote_copy(
            src_ref=ref, dst_ref=ref, send_sem=sib_ss.at[blk], recv_sem=sib_rs.at[blk],
            device_id=sib, device_id_type=pl.DeviceIdType.MESH)

    def x_copy(blk, parity, side):
        ref = pf.at[blk, c, pl.ds(pl.multiple_of(parity * quarter, 16) + side * (quarter // 2), quarter // 2)]
        return pltpu.make_async_remote_copy(
            src_ref=ref, dst_ref=ref, send_sem=x_ss.at[side, blk], recv_sem=x_rs.at[side, blk],
            device_id={TP: ((t // 2 + (1, 3)[side]) % SIDE) * 2 + c}, device_id_type=pl.DeviceIdType.MESH)

    def to_x(*blks):
        for blk in blks:
            for side in (0, 1):
                cp = x_copy(blk, par, side)
                cp.start()
                sent.append(cp)

    def from_x(*blks):
        for blk in blks:
            for side in (0, 1):
                x_copy(blk, 1 - par, side).wait_recv()
            cp = sib_copy(blk, c)
            cp.start()
            sent.append(cp)

    pg.start()

    for cp in own_f32:
        cp.wait()
    row = 0
    for src in (wq, wo, fq, fo, sq, so):
        for col in range(0, src.shape[1], 128):
            part = src[:, col:col + 128]
            if src is wq or src is wo:
                part = part * (1.0 - step_rate * decay_rate)
            pw[i, row:row + src.shape[0], :] = part.astype(BF16)
            row += src.shape[0]

    def w_stage(w, s):
        g = wgs[w]
        if s == 0:
            g.start()
        elif s == 1:
            g.take_a(1)
            g.take_a(2)
        elif s == 2:
            g.take_b(0)
            g.take_a2()
        elif s == 3:
            g.take_b(1)
            g.take_b(2)
        elif s == 4:
            g.take_b(3)
        else:
            for m in range(4):
                g.take_b2(m)

    def transposes():
        l_ho.wait()
        ho_t[...] = ho[...].T
        l_gq.wait()
        gq_t[...] = gq[...].T

    def gradient_o(k):
        if k % 4 == 0:
            l_go[k // 4].wait()
        grad_o[:, k * 256:k * 256 + 256] = dot(ho_t[...], go[:, k * 256:k * 256 + 256]).astype(BF16)

    def gradient_q(k):
        if k == 0:
            l_xq.wait()
        grad_q[:, k * 256:k * 256 + 256] = dot(gq_t[...], xq[:, k * 256:k * 256 + 256]).astype(BF16)

    def wait_sib(*blks):
        for blk in blks:
            sib_copy(blk, 1 - c).wait_recv()

    def project_o(*blks):
        out = None
        for blk in blks:
            p = pf[blk].reshape(2 * half, -1)[nq:]
            d = dot(grad_o[:, pl.ds(pl.multiple_of(blk * no, no), no)], p)
            out = d if out is None else out + d
        return out

    a1, a2, a3 = (a + 3) % SIDE, (a + 1) % SIDE, (a + 2) % SIDE
    b1, b2, b3 = (b + 3) % SIDE, (b + 1) % SIDE, (b + 2) % SIDE
    near = [fs_of(p, q) for p in (a1, a2) for q in (b1, b2)] + [fs_of(a, b1), fs_of(a, b2), fs_of(a1, b), fs_of(a2, b)]
    far = [fs_of(a3, b), fs_of(a, b3), fs_of(a3, b1), fs_of(a3, b2), fs_of(a1, b3), fs_of(a2, b3)]
    last = fs_of(a3, b3)

    def project_near():
        wait_sib(*near)
        acc[...] = project_o(i, *near)

    cq = fq.shape[1]

    zs, ys, ts = [(z + d) % SIDE for d in range(SIDE)], [(y + d) % SIDE for d in range(SIDE)], []
    for d in range(N_TP):
        ts.append(((t // 2 + d // 2) % SIDE) * 2 + (c + d % 2) % 2)
    distance = lambda d: sum(min(k, SIDE - k) for k in (d[0], d[1], d[2] // 2)) * 2 + d[2] % 2
    far_first = sorted(((dz, dy, dt) for dz in range(SIDE) for dy in range(SIDE) for dt in range(N_TP)),
                       key=distance, reverse=True)[:-1]
    plane_far_first = [(dz, dy) for dz, dy, dt in far_first if dt == 0]

    def rs_copy(dz, dy):
        d, to = dz * SIDE + dy, zs[dz] * SIDE + ys[dy]
        return pltpu.make_async_remote_copy(
            src_ref=rs_out.at[to], dst_ref=rs_in.at[d], send_sem=rs_ss.at[d], recv_sem=rs_rs,
            device_id={FS: to}, device_id_type=pl.DeviceIdType.MESH)

    def project_q(*zrows):
        out = None
        for zr in zrows:
            p = pf[pl.ds(zr * SIDE, SIDE), 0, 0:nq, :].reshape(SIDE * nq, -1)
            d = dot(grad_q[:, pl.ds(pl.multiple_of(zr * SIDE * nq, SIDE * nq), SIDE * nq)], p)
            out = d if out is None else out + d
        return out

    def project_far():
        wait_sib(*far)
        acc[...] += project_o(*far)
        acc_q[...] = project_q(z, (z + 1) % SIDE, (z + 3) % SIDE)

    def send_partials():
        wait_sib(last)
        part_o = acc[...] + project_o(last)
        part_q = acc_q[...] + project_q((z + 2) % SIDE)
        rs_out[:, :, cq:] = part_o.T.astype(BF16).reshape(N_FS, -1, part_o.shape[0])
        rs_out[:, :, :cq] = part_q.T.astype(BF16).reshape(N_FS, -1, part_q.shape[0])
        for dz, dy in plane_far_first:
            rs_copy(dz, dy).start()

    me = i * N_TP + t

    def ag_copy(dz, dy, back=False):
        d, to = dz * SIDE + dy, zs[dz] * SIDE + ys[dy]
        ref = lowg.at[zs[-dz] * SIDE + ys[-dy] if back else i]
        return pltpu.make_async_remote_copy(
            src_ref=ref, dst_ref=ref, send_sem=ag_ss.at[d], recv_sem=ag_rs.at[d],
            device_id={FS: to}, device_id_type=pl.DeviceIdType.MESH)

    def lows():
        for dz, dy in plane_far_first:
            ag_copy(dz, dy, back=True).wait_recv()

    others = sums.at[pl.ds(0, N_FS * N_TP - 1)]

    def reduce_partials():
        arrived = rs_in.at[pl.ds(1, N_FS - 1)]
        pltpu.make_async_copy(arrived, arrived, rs_rs).wait()
        reduced = rs_out[i].astype(F32)
        for d in range(1, N_FS):
            reduced = reduced + rs_in[d].astype(F32)
        low[...] = reduced
        lowg[i] = reduced.astype(BF16)
        sums[me] = jnp.full(sums.shape[1:], jnp.sum(reduced * reduced), F32)
        for dz, dy, dt in far_first:
            pltpu.make_async_remote_copy(
                src_ref=sums.at[me], dst_ref=sums.at[me], send_sem=sum_ss, recv_sem=sum_rs,
                device_id={FS: zs[dz] * SIDE + ys[dy], TP: ts[dt]}, device_id_type=pl.DeviceIdType.MESH).start()
        for dz, dy in plane_far_first:
            ag_copy(dz, dy).start()

    def clip():
        pltpu.make_async_copy(others, others, sum_rs).wait()
        scale[...] = jnp.broadcast_to(
            jnp.minimum(1.0, target / jnp.sqrt(jnp.sum(sums[...], axis=0))), scale.shape)

    along_a = [a, a1, a2, a3]
    steps = dict(a=lambda m: to_x(pg.take_a(m) if m < 3 else pg.take_a2()), b=lambda m: to_x(*pg.take_b(m)),
                 c=lambda m: to_x(pg.take_b2(m)), xa=lambda m: from_x(fs_of(along_a[m], b)),
                 xb=lambda m: from_x(fs_of(along_a[m], b1), fs_of(along_a[m], b2)),
                 xc=lambda m: from_x(fs_of(along_a[m], b3)), w=w_stage, t=transposes, g=gradient_o, q=gradient_q, near=project_near, far=project_far,
                 send=send_partials, reduce=reduce_partials, clip=clip,
                 lows=lows)
    for name, *args in ORDER:
        steps[name](*args)
    pltpu.make_async_copy(others, others, sum_ss).wait()
    for g in [pg] + wgs:
        g.finish()
    for cp in sent:
        cp.wait_send()
    for dz, dy in plane_far_first:
        rs_copy(dz, dy).wait_send()
    for dz, dy in plane_far_first:
        ag_copy(dz, dy).wait_send()


def update_kernel(pf, pw, lowg, low, scale, pq, po, wq, wo, fq, sq, fo, so, *refs):
    held, (dirs, *bufs, sems) = refs[:10], refs[10:]
    nwq, nwo, nfq, nsq, nfo, nso, stq, sto, cpq, cpo = bufs
    cq, co = fq.shape[1], fo.shape[1]
    nq, no, rows = pq.shape[0], po.shape[0], fq.shape[0]
    n = N_FS // CHUNKS
    blocks = (cq + co) // 128
    at_o = (cq // 128) * nq
    at_f = at_o + (co // 128) * no
    s = scale[0:1, 0:1]
    outgoing = []

    def write(k, part=None):
        src, dst = bufs[k], held[k]
        if part is not None:
            src, dst = src.at[part], dst.at[part]
        cp = pltpu.make_async_copy(src, dst, sems.at[len(outgoing)])
        cp.start()
        outgoing.append(cp)

    for j in range(blocks):
        f = pw[:, at_f + j * rows:at_f + (j + 1) * rows, :].astype(F32)
        v = pw[:, at_f + (blocks + j) * rows:at_f + (blocks + j + 1) * rows, :].astype(F32)
        l = lowg[:, :, j * 128:(j + 1) * 128].astype(F32)
        d = moments(f, v, l, s)[2]
        dirs[:, j * 128:(j + 1) * 128] = (-step_rate * d).reshape(-1, 128).astype(BF16)
    dq, do = dirs[:, :cq], dirs[:, cq:]

    for g in range(CHUNKS):
        own = slice(g * n, (g + 1) * n)
        whole = pf[own].reshape(n, nq + no, pf.shape[3])
        mo = dot(whole[:, nq:, :].reshape(n * no, -1), do)
        at = pl.ds(g * n * no, n * no)
        for col in range(0, co, 128):
            lo = at_o + (col // 128) * no
            w = pw[own, lo:lo + no, :].astype(F32).reshape(n * no, 128)
            cpo[at, col:col + 128] = (w + mo[:, col:col + 128]).astype(BF16)
        write(9, at)
        mq = dot(whole[:, :nq, :].reshape(n * nq, -1), dq)
        at = pl.ds(g * n * nq, n * nq)
        for col in range(0, cq, 128):
            w = pw[own, (col // 128) * nq:(col // 128 + 1) * nq, :].astype(F32).reshape(n * nq, 128)
            cpq[at, col:col + 128] = (w + mq[:, col:col + 128]).astype(BF16)
        write(8, at)
        if g == 0:
            for p_, d_, w_, st_, nw_ in ((pq, dq, wq, stq, nwq), (po, do, wo, sto, nwo)):
                step = dot(p_[...], d_) * (-1.0 / step_rate) + decay_rate * w_[...]
                st_[...] = step
                nw_[...] = w_[...] - step_rate * step
            for k in (6, 7, 0, 1):
                write(k)
            nfq[...], nsq[...], _ = moments(fq[...], sq[...], low[:, :cq], s)
            nfo[...], nso[...], _ = moments(fo[...], so[...], low[:, cq:], s)
            for k in (2, 3, 4, 5):
                write(k)
    for cp in outgoing:
        cp.wait()


def per_device(query_latent_rows, grad_q, head_out, grad_out, proj_q, proj_o, query_up_weight, weight_o,
               first_q, second_q, first_o, second_o):
    nq, no, rank = proj_q.shape[0], proj_o.shape[0], proj_q.shape[1]
    cq, co = first_q.shape[1], first_o.shape[1]
    rows = first_q.shape[0]
    target = math.sqrt(rows * N_FS * (cq + co) * N_TP)
    half = (nq + no) // 2
    wrows = (nq * cq + no * co + 2 * rows * (cq + co)) // 128
    sds = jax.ShapeDtypeStruct
    dma = pltpu.SemaphoreType.DMA
    V = pltpu.VMEM
    ins = (query_latent_rows, grad_q, head_out, grad_out, proj_q, proj_o, query_up_weight, weight_o,
           first_q, second_q, first_o, second_o)
    like = lambda x: V(x.shape, x.dtype)
    tokens = query_latent_rows.shape[0]

    def ex(*refs):
        exchange_kernel(target, *refs)

    gathered = pl.pallas_call(
        ex,
        out_shape=[V((N_FS, 2, half, rank), BF16), V((N_FS, wrows, 128), BF16),
                   V((N_FS, rows, cq + co), BF16), V((rows, cq + co), F32), V((8, 128), F32)],
        in_specs=[pl.BlockSpec(memory_space=pltpu.HBM)] * len(ins),
        out_specs=[pl.BlockSpec(memory_space=pltpu.VMEM)] * 5,
        scratch_shapes=[
            like(query_latent_rows), like(grad_q), like(head_out), like(grad_out),
            like(query_up_weight), like(weight_o), like(first_q), like(second_q), like(first_o), like(second_o),
            V((co, tokens), BF16), V((cq, tokens), BF16), V((co, N_FS * no), BF16), V((cq, N_FS * nq), BF16),
            V((co, rank), F32), V((cq, rank), F32), V((N_FS, rows, cq + co), BF16), V((N_FS, rows, cq + co), BF16),
            V((N_FS * N_TP, 1, 128), F32),
            dma((16,)), dma((20,)), dma((20,)), dma((NW, 20)), dma((NW, 20)),
            dma((N_FS,)), dma((N_FS,)), dma((2, N_FS)), dma((2, N_FS)),
            dma((N_FS,)), dma, dma, dma, dma((N_FS,)), dma((N_FS,)),
        ],
        compiler_params=pltpu.CompilerParams(collective_id=0, has_side_effects=True,
                                             vmem_limit_bytes=48 * 1024 * 1024),
        name="exchange",
    )(*[pltpu.with_memory_space_constraint(x, pltpu.HBM) for x in ins])

    outs = [sds((nq, cq), F32), sds((no, co), F32), sds((rows, cq), F32), sds((rows, cq), F32),
            sds((rows, co), F32), sds((rows, co), F32), sds((nq, cq), F32), sds((no, co), F32),
            sds((N_FS * nq, cq), BF16), sds((N_FS * no, co), BF16)]
    ops = (*gathered, proj_q, proj_o, query_up_weight, weight_o, first_q, second_q, first_o, second_o)
    return tuple(pl.pallas_call(
        update_kernel,
        in_specs=[pl.BlockSpec(memory_space=pltpu.VMEM)] * len(ops),
        out_specs=[pl.BlockSpec(memory_space=pltpu.HBM)] * len(outs),
        out_shape=outs,
        scratch_shapes=[V((rows * N_FS, cq + co), BF16)] + [like(o) for o in outs] + [dma((8 + 2 * CHUNKS,))],
        compiler_params=pltpu.CompilerParams(vmem_limit_bytes=24 * 1024 * 1024),
        name="update",
    )(*ops))


def solution(mesh):
    rows, both, cols = P(FS, None), P(FS, TP), P(None, TP)
    return jax.shard_map(
        per_device,
        mesh=mesh,
        in_specs=(rows, both, both, rows, rows, rows) + (both,) * 6,
        out_specs=(both,) * 8 + (cols, cols),
        check_vma=False,
    )
```
